32 devices in a mesh: grp: 2 (over y), sp: 4 (over z), fs: 2 (over x), tp: 2 (over core).
Axes of the slice: x: 2, y: 2, z: 4, core: 2. Of those that a mesh axis runs over, the one named last changes fastest.
Arguments:
- tokens: bfloat16 [4, 1024, 2048], P(('grp', 'fs'), 'sp', 'tp'), parts along dimension 0, may hold values from -6 to 6
- input_norm_gain: float32 [2048], replicated, may hold values from 0.1 to 1.9
- query_weight: bfloat16 [2048, 1024], P('sp', 'tp'), may hold values from -0.125 to 0.125
- key_weight: bfloat16 [2048, 1024], P('sp', 'tp'), may hold values from -0.125 to 0.125
- value_weight: bfloat16 [2048, 1024], P('sp', 'tp'), may hold values from -0.125 to 0.125
- decay_gate_weight: bfloat16 [2048, 8], replicated, may hold values from -0.125 to 0.125
- write_strength_weight: bfloat16 [2048, 8], replicated, may hold values from -0.125 to 0.125
- up_weight: bfloat16 [2048, 1024], P('sp', 'tp'), may hold values from -0.125 to 0.125
- gate_half_weight: bfloat16 [2048, 1024], P('sp', 'tp'), may hold values from -0.125 to 0.125
- log_decay_rate: float32 [8], replicated, may hold values from -30 to 0
- write_strength_bias: float32 [8], replicated, may hold values from -7 to 1
- decay_spike_added: float32 [4, 1024, 8], P(('grp', 'fs'), 'sp', 'tp'), parts along dimension 0, may hold values from -2 to 0
- starting_state: float32 [4, 8, 128, 128], P(('grp', 'fs'), 'tp'), parts along dimension 0, may hold values from -4 to 4
- head_norm_gain: float32 [128], replicated, may hold values from 0.1 to 1.9
- convolution_kernel: float32 [31, 1024], replicated, may hold values from -4 to 4
- channel_norm_gain: float32 [1024], replicated, may hold values from 0.1 to 1.9
- delta_output_rows: bfloat16 [1024, 2048], P('tp', 'sp'), may hold values from -0.125 to 0.125
- convolution_output_rows: bfloat16 [1024, 2048], P('tp', 'sp'), may hold values from -0.125 to 0.125
Outputs:
- mixed: bfloat16 [4, 1024, 2048], P(('grp', 'fs'), 'sp', 'tp'), parts along dimension 0
The draws below stay inside these ranges and needn't reach their ends.
There are 2 independent parts, one for each index of `grp`. The reference program is written for one: setup_inputs(seed, part) draws one part's arguments, and reference() takes and returns one part's arrays. A program takes and returns all parts, laid end to end along the dimension named above; an argument that names none is the same for every part. Nothing has to cross between parts.
All inputs are finite; a program needn't handle non-finite values.
Results may differ from the reference program's by a relative error of at most 0.01.
Values may be sent and summed in bfloat16 or wider, within the bound.
A program may use at most 64 MiB of HBM per device.

```python
import math
import jax
import jax.numpy as jnp
from jax import lax

D = 2048
HEADS = 8
HEAD = 128
CH = 1024
KSIZE = 31
BLOCK = 64
TOK_DEV = 256
LEN = 1024
SEQS = 2
WIDTH_A = 1024
N_TP = 2


def fast_heads(key, fast_count):
    order = jax.random.permutation(jax.random.fold_in(key, 11), HEADS)
    return order < fast_count


def draw_log_decay_rate(key, part):
    fast_key = jax.random.fold_in(key, 12)
    slow_key = jax.random.fold_in(key, 13)
    fast_count = HEADS // 2
    fast_mask = fast_heads(key, fast_count)
    fast_rate = jnp.exp(jax.random.uniform(fast_key, (HEADS,), jnp.float32, math.log(1.0 / 60.0), math.log(1.0 / 30.0))) / 0.7
    slow_rate = 0.5 / (0.7 * LEN) * jnp.exp(jax.random.uniform(slow_key, (HEADS,), jnp.float32, math.log(0.5), 0.0))
    return jnp.log(jnp.where(fast_mask, fast_rate, slow_rate)).astype(jnp.float32)


def draw_write_strength_bias(key, part):
    fast_key = jax.random.fold_in(key, 31)
    slow_key = jax.random.fold_in(key, 32)
    fast_count = HEADS // 2
    fast_mask = fast_heads(key, fast_count)
    fast_level = jax.random.uniform(fast_key, (HEADS,), jnp.float32, -1.0, 1.0)
    slow_level = math.log(0.5 * HEAD / LEN) + jax.random.uniform(slow_key, (HEADS,), jnp.float32, math.log(0.5), 0.0)
    return jnp.where(fast_mask, fast_level, slow_level).astype(jnp.float32)


def draw_decay_spike_added(key, part):
    level_key = jax.random.fold_in(key, 21)
    place_key = jax.random.fold_in(key, 22)
    depth_key = jax.random.fold_in(key, 23)
    blocks = LEN // TOK_DEV
    decay_levels = jax.random.uniform(level_key, (SEQS, blocks, HEADS), jnp.float32, 0.0, 1.0) * (-1.0 / LEN)
    decay_levels = jnp.repeat(decay_levels, TOK_DEV, axis=1)
    places = jax.random.randint(place_key, (SEQS, 2, HEADS), 0, LEN)
    sequence_depths = jnp.log(jax.random.uniform(depth_key, (SEQS, 2, HEADS), jnp.float32, 0.6, 0.8))
    positions = jnp.arange(LEN, dtype=jnp.int32)
    spike_applied = positions[None, :, None, None] == places[:, None, :, :]
    decay_spikes = jnp.sum(jnp.where(spike_applied, sequence_depths[:, None, :, :], 0.0), axis=2)
    return (decay_levels + decay_spikes).astype(jnp.float32)


def draw_convolution_kernel(key, part):
    raw = jnp.clip(jax.random.normal(key, (KSIZE, CH), jnp.float32), -6.0, 6.0)
    channel = jnp.arange(CH, dtype=jnp.float32) / CH
    scales = jnp.exp(math.log(10.0) * channel - 0.5 * math.log(10.0))
    return (raw * KSIZE ** (-0.5) * scales[None, :]).astype(jnp.float32)


def steps_of(stream_key, extent, split, least, largest):
    gain = 1.0
    for dim, shards_of in split:
        steps = jax.random.uniform(jax.random.fold_in(jax.random.fold_in(stream_key, 6), dim), (shards_of,), jnp.float32, least / len(split), largest / len(split))
        gain = gain * jnp.repeat(jnp.exp(steps), extent[dim] // shards_of).reshape((-1,) + (1,) * (len(extent) - 1 - dim))
    return gain


def bell_draw(own_key, dims, width, most, pieces=(), kind=jnp.bfloat16):
    result = width * jax.random.normal(own_key, dims, jnp.float32)
    if pieces:
        result = result * steps_of(own_key, dims, pieces, -0.22, 0.18)
    return jnp.clip(result, -most, most).astype(kind)


def setup_inputs(seed: int = 0, part: int = 0) -> dict:
    splits = jax.random.split(jax.random.key(seed), 19)
    part_keys = jax.random.split(jax.random.fold_in(splits[18], part), 19)
    tokens = bell_draw(part_keys[0], (SEQS, LEN, D), 1.0, 6.0, ((0, 2), (1, 4), (2, 2)))
    input_norm_gain = jnp.clip(1.0 + 0.18 * jax.random.normal(splits[1], (D,), jnp.float32), 0.1, 1.9)
    query_weight = bell_draw(splits[2], (D, WIDTH_A), D ** -0.5, 0.125, ((0, 4), (1, 2)))
    key_weight = bell_draw(splits[3], (D, WIDTH_A), D ** -0.5, 0.125, ((0, 4), (1, 2)))
    value_weight = bell_draw(splits[4], (D, WIDTH_A), D ** -0.5, 0.125, ((0, 4), (1, 2)))
    decay_gate_weight = bell_draw(splits[5], (D, HEADS), D ** -0.5, 0.125)
    write_strength_weight = bell_draw(splits[6], (D, HEADS), D ** -0.5, 0.125)
    up_weight = bell_draw(splits[7], (D, CH), D ** -0.5, 0.125, ((0, 4), (1, 2)))
    gate_half_weight = bell_draw(splits[8], (D, CH), D ** -0.5, 0.125, ((0, 4), (1, 2)))
    log_decay_rate = draw_log_decay_rate(jax.random.fold_in(splits[18], 71), part)
    write_strength_bias = draw_write_strength_bias(jax.random.fold_in(splits[18], 71), part)
    decay_spike_added = draw_decay_spike_added(jax.random.fold_in(jax.random.fold_in(splits[18], part), 71), part)
    starting_state = bell_draw(part_keys[12], (SEQS, HEADS, HEAD, HEAD), 0.5, 4.0, ((0, 2), (1, 2)), jnp.float32)
    head_norm_gain = jnp.clip(1.0 + 0.18 * jax.random.normal(splits[13], (HEAD,), jnp.float32), 0.1, 1.9)
    convolution_kernel = draw_convolution_kernel(jax.random.fold_in(splits[18], 71), part)
    channel_norm_gain = jnp.clip(1.0 + 0.18 * jax.random.normal(splits[15], (CH,), jnp.float32), 0.1, 1.9)
    delta_output_rows = bell_draw(splits[16], (WIDTH_A, D), (WIDTH_A + CH) ** -0.5, 0.125, ((0, 2), (1, 4)))
    convolution_output_rows = bell_draw(splits[17], (CH, D), (WIDTH_A + CH) ** -0.5, 0.125, ((0, 2), (1, 4)))
    return dict(tokens=tokens, input_norm_gain=input_norm_gain, query_weight=query_weight, key_weight=key_weight, value_weight=value_weight, decay_gate_weight=decay_gate_weight, write_strength_weight=write_strength_weight, up_weight=up_weight, gate_half_weight=gate_half_weight, log_decay_rate=log_decay_rate, write_strength_bias=write_strength_bias, decay_spike_added=decay_spike_added, starting_state=starting_state, head_norm_gain=head_norm_gain, convolution_kernel=convolution_kernel, channel_norm_gain=channel_norm_gain, delta_output_rows=delta_output_rows, convolution_output_rows=convolution_output_rows)


EPS = 1e-06
HIGH = lax.Precision.HIGHEST

def unit_rows(values):
    return values * lax.rsqrt(lax.optimization_barrier(jnp.sum(values * values, axis=-1, keepdims=True)) + EPS)

def rounded(values):
    return lax.optimization_barrier(values.astype(jnp.bfloat16)).astype(jnp.float32)

def block_terms(query, keys, values, log_decay, beta):
    rows = keys.shape[0]
    count = rows // BLOCK

    def split_blocks(array):
        return jnp.swapaxes(array.reshape((count, BLOCK) + array.shape[1:]), 1, 2)
    q_blocks, k_blocks, v_blocks = (split_blocks(query), split_blocks(keys), split_blocks(values))
    g_blocks, b_blocks = (split_blocks(log_decay), split_blocks(beta))
    cumdec = jnp.cumsum(g_blocks, axis=-1)
    lower = jnp.tril(jnp.ones((BLOCK, BLOCK), bool))
    strict = jnp.tril(jnp.ones((BLOCK, BLOCK), bool), -1)
    diff = cumdec[..., :, None] - cumdec[..., None, :]
    gamma = jnp.where(lower, jnp.exp(jnp.where(lower, diff, 0.0)), 0.0)
    k_beta = k_blocks * b_blocks[..., None]
    a_matrix = jnp.where(strict, jnp.einsum('nhid,nhjd->nhij', k_beta, k_blocks, precision=HIGH) * gamma, 0.0)
    left_side = a_matrix + jnp.eye(BLOCK, dtype=jnp.float32)
    right_side = jnp.concatenate([v_blocks * b_blocks[..., None], k_beta * jnp.exp(cumdec)[..., None]], axis=-1)
    solved = jax.scipy.linalg.solve_triangular(left_side, right_side, lower=True, unit_diagonal=True)
    width_v = v_blocks.shape[-1]
    updates, w_rows = (solved[..., :width_v], solved[..., width_v:])
    q_k = jnp.where(lower, jnp.einsum('nhid,nhjd->nhij', q_blocks, k_blocks, precision=HIGH) * gamma, 0.0)
    last = cumdec[..., -1]
    k_decayed = k_blocks * jnp.exp(last[..., None] - cumdec)[..., None]
    q_decayed = q_blocks * jnp.exp(cumdec)[..., None]
    return (q_decayed, k_decayed, updates, w_rows, q_k, last)

def block_outputs(start_state, terms):

    def advance(state, input_rows):
        q_decayed, k_decayed, updates, w_rows, q_k, last = input_rows
        v_new = updates - jnp.einsum('hcd,hde->hce', w_rows, state, precision=HIGH)
        output = jnp.einsum('hcd,hde->hce', q_decayed, state, precision=HIGH) + jnp.einsum('hij,hje->hie', q_k, v_new, precision=HIGH)
        state = state * jnp.exp(last)[..., None, None] + jnp.einsum('hcd,hce->hde', k_decayed, v_new, precision=HIGH)
        return (state, output)
    _, outputs = lax.scan(advance, start_state, terms)
    count, heads, blen, width_v = outputs.shape
    return jnp.swapaxes(outputs, 1, 2).reshape(count * blen, heads, width_v)

def single_sequence(tokens, decay_spike_added, starting_state, input_norm_gain, query_weight, key_weight, value_weight, decay_gate_weight, write_strength_weight, up_weight, gate_half_weight, log_decay_rate, write_strength_bias, head_norm_gain, convolution_kernel, channel_norm_gain, delta_output_rows, convolution_output_rows):
    rows = tokens.shape[0]
    token_f = tokens.astype(jnp.float32)
    normed = (token_f * lax.rsqrt(lax.optimization_barrier(jnp.mean(token_f * token_f, axis=-1, keepdims=True)) + EPS) * input_norm_gain).astype(jnp.bfloat16)

    def project_input(weight):
        return rounded(jnp.dot(normed.astype(jnp.float32), weight.astype(jnp.float32), preferred_element_type=jnp.float32))
    shape = (rows, HEADS, HEAD)
    query = unit_rows(jax.nn.silu(project_input(query_weight)).reshape(shape)) * HEAD ** (-0.5)
    keys = unit_rows(jax.nn.silu(project_input(key_weight)).reshape(shape))
    values = jax.nn.silu(project_input(value_weight)).reshape(shape)
    log_decay = -jnp.exp(log_decay_rate) * jax.nn.softplus(project_input(decay_gate_weight)) + decay_spike_added
    beta = jax.nn.sigmoid(project_input(write_strength_weight) + write_strength_bias)
    terms = block_terms(query, keys, values, log_decay, beta)
    attn = block_outputs(starting_state, terms)
    attn_out = (attn * lax.rsqrt(lax.optimization_barrier(jnp.mean(attn * attn, axis=-1, keepdims=True)) + EPS) * head_norm_gain).astype(jnp.bfloat16)
    attn_out = attn_out.reshape(rows, HEADS * HEAD)
    glu = lax.optimization_barrier((project_input(up_weight) * jax.nn.sigmoid(project_input(gate_half_weight))).astype(jnp.bfloat16))
    padded = jnp.concatenate([jnp.zeros((KSIZE - 1, CH), jnp.float32), glu.astype(jnp.float32)], axis=0)
    conv = jnp.zeros((rows, CH), jnp.float32)
    for tap in range(KSIZE):
        conv = conv + convolution_kernel[tap] * padded[tap:tap + rows]
    mean_c = lax.optimization_barrier(jnp.mean(conv, axis=-1, keepdims=True))
    var_c = lax.optimization_barrier(jnp.mean(conv * conv, axis=-1, keepdims=True)) - mean_c * mean_c
    conv_out = jax.nn.silu((conv - mean_c) * lax.rsqrt(var_c + EPS) * channel_norm_gain).astype(jnp.bfloat16)
    attn_group = HEADS * HEAD // N_TP
    conv_group = CH // N_TP
    total = jnp.zeros((rows, D), jnp.float32)
    for group in range(N_TP):
        partial_value = jnp.dot(attn_out[:, group * attn_group:(group + 1) * attn_group].astype(jnp.float32), delta_output_rows[group * attn_group:(group + 1) * attn_group].astype(jnp.float32), preferred_element_type=jnp.float32)
        partial_value = partial_value + jnp.dot(conv_out[:, group * conv_group:(group + 1) * conv_group].astype(jnp.float32), convolution_output_rows[group * conv_group:(group + 1) * conv_group].astype(jnp.float32), preferred_element_type=jnp.float32)
        total = total + rounded(partial_value)
    return total.astype(jnp.bfloat16)

def reference(tokens, input_norm_gain, query_weight, key_weight, value_weight, decay_gate_weight, write_strength_weight, up_weight, gate_half_weight, log_decay_rate, write_strength_bias, decay_spike_added, starting_state, head_norm_gain, convolution_kernel, channel_norm_gain, delta_output_rows, convolution_output_rows):

    def sequence_wise(input_rows):
        sequence_token, sequence_spike, sequence_state = input_rows
        return single_sequence(sequence_token, sequence_spike, sequence_state, input_norm_gain, query_weight, key_weight, value_weight, decay_gate_weight, write_strength_weight, up_weight, gate_half_weight, log_decay_rate, write_strength_bias, head_norm_gain, convolution_kernel, channel_norm_gain, delta_output_rows, convolution_output_rows)
    return lax.map(sequence_wise, (tokens, decay_spike_added, starting_state))
```

```python
import functools

import jax
import jax.numpy as jnp
from jax import lax
from jax.experimental import pallas as pl
from jax.experimental.pallas import tpu as pltpu
from jax.sharding import PartitionSpec as P

HEAD = 128
CHUNK = 128
EPS = 1e-06
HIGH = lax.Precision.HIGHEST
MESH = pl.DeviceIdType.MESH
F32 = jnp.float32
BF16 = jnp.bfloat16


def dot(a, b, dims, precision=None):
    return lax.dot_general(a, b, (dims, ((), ())), preferred_element_type=F32, precision=precision)


def mm(a, b, precision=None):
    return dot(a, b, ((1,), (0,)), precision)


def mm_nt(a, b, precision=None):
    return dot(a, b, ((1,), (1,)), precision)


def mm_tn(a, b, precision=None):
    return dot(a, b, ((0,), (0,)), precision)


def split(x):
    high = x.astype(BF16)
    return high, (x - high.astype(F32)).astype(BF16)


def mm3(a, b, form=mm):
    a_high, a_low = split(a)
    b_high, b_low = split(b)
    return form(a_high, b_high) + (form(a_high, b_low) + form(a_low, b_high))


def mm1(a, b, form=mm):
    return form(a.astype(BF16), b.astype(BF16))


def silu(x):
    return x * jax.nn.sigmoid(x)


def unit(x):
    return x * lax.rsqrt(jnp.sum(x * x, axis=-1, keepdims=True) + EPS)


def softplus(x):
    return jnp.maximum(x, 0.0) + jnp.log1p(jnp.exp(-jnp.abs(x)))


def aligned(index, size):
    return pl.ds(pl.multiple_of(index * size, size), size)


def layer_kernel(
    sizes,
    tok_ref, wq_ref, wk_ref, wv_ref, wu_ref, wg_ref, wd_ref, wc_ref,
    spike_ref, state_ref, gates_ref, gain_ref, rate_ref, bias_ref, head_gain_ref, taps_ref, chan_gain_ref,
    out_ref,
    tok_all, normed, w_all, wo_all, raw, spikes, small, rows_ref, cols_ref,
    t_all, k_all, gamma_all, p_all, u_all, m_all, o_all, p_out, u_out, x_end,
    st_first, st_send, st_recv, ext, tail, rim, conv_ref, stat_ref, sums, mix,
    to_pair, from_pair, to_z, from_z, own_sum,
    z_send, z_recv, x_send, x_recv, y_send, y_recv, a_send, a_recv, b_send, b_recv,
    tok_sem_s, tok_sem_r, misc_s, misc_r, sum_s, sum_r, pair_s, pair_r, zo_s, zo_r, local_sem,
):
    across, ring, down = sizes
    rows, half = tok_ref.shape
    depth, wide_tp = wq_ref.shape
    wide = wide_tp // 2
    heads = wide // HEAD
    pos = 2 * rows
    chunks = pos // CHUNK
    shard = wd_ref.shape[1]
    lines = down * across
    piece = depth // lines
    out_piece = wide // lines
    tap_count = taps_ref.shape[0]
    channels = taps_ref.shape[1]
    pad = ext.shape[0] - pos

    g, s, f, t = (lax.axis_index(name) for name in ("grp", "sp", "fs", "tp"))
    b = lax.rem(s, 2)
    line = g * across + f
    z_at = lambda j: {"sp": lax.rem(s + j, ring)}
    x_at = lambda a: {"fs": lax.rem(f + a, across)}
    y_at = lambda c: {"grp": lax.rem(g + c, down)}
    partner = {"tp": 1 - t}
    z_peer = {"sp": s + 1 - 2 * b}
    far = {"sp": s + 1 - 2 * b, "tp": 1 - t}
    ahead = {"sp": lax.rem(s + 2, ring)}
    z_span, x_span, y_span = range(1, ring), range(1, across), range(1, down)

    def copy(src, dst, send_sem, recv_sem, peer):
        return pltpu.make_async_remote_copy(
            src_ref=src, dst_ref=dst, send_sem=send_sem, recv_sem=recv_sem, device_id=peer, device_id_type=MESH
        )

    weights = (wk_ref, wq_ref, wv_ref, wu_ref, wg_ref)
    out_weights = (wd_ref, wc_ref)
    OUT = len(weights)

    local = [pltpu.make_async_copy(tok_ref, tok_all.at[b, :, aligned(t, half)], local_sem.at[0])]
    local.append(pltpu.make_async_copy(spike_ref, spikes.at[b], local_sem.at[1]))
    for i, w in enumerate(weights):
        local.append(
            pltpu.make_async_copy(w.at[:, aligned(b, wide)], w_all.at[i, aligned(s, depth), :], local_sem.at[2 + i])
        )
    for i, w in enumerate(out_weights):
        local.append(
            pltpu.make_async_copy(w.at[aligned(b, wide), :], wo_all.at[i, :, aligned(s, shard)], local_sem.at[2 + OUT + i])
        )
    for one in local:
        one.start()

    barrier = pltpu.get_barrier_semaphore()
    friends = [z_at(j) for j in z_span] + [x_at(a) for a in x_span] + [y_at(c) for c in y_span] + [partner, far]
    for friend in friends:
        pl.semaphore_signal(barrier, inc=1, device_id=friend, device_id_type=MESH)
    pl.semaphore_wait(barrier, len(friends))

    z_copies = {}

    def z_send_piece(i):
        for j in z_span:
            to = lax.rem(lax.rem(s + j, ring), 2)
            if i < OUT:
                src = weights[i].at[aligned(line, piece), aligned(to, wide)]
                dst = w_all.at[i, pl.ds(pl.multiple_of(s * depth + line * piece, piece), piece), :]
            else:
                begin = pl.multiple_of(to * wide + line * out_piece, out_piece)
                src = out_weights[i - OUT].at[pl.ds(begin, out_piece), :]
                dst = wo_all.at[i - OUT, aligned(line, out_piece), aligned(s, shard)]
            one = copy(src, dst, z_send.at[i, j - 1], z_recv.at[i, j - 1], z_at(j))
            one.start()
            z_copies[i, j] = one

    part = rows // 2
    toks = {}

    def tok_place(side, h, from_tp):
        return tok_all.at[side, pl.ds(h * part, part), aligned(from_tp, half)]

    def tok_z(h):
        toks[h] = copy(
            tok_ref.at[pl.ds(h * part, part), :], tok_place(b, h, t), tok_sem_s.at[h], tok_sem_r.at[h], z_peer
        )
        toks[h].start()

    to_partner = copy(tok_ref, tok_all.at[b, :, aligned(t, half)], tok_sem_s.at[4], tok_sem_r.at[4], partner)
    to_partner.start()
    spike_copy = copy(spike_ref, spikes.at[b], misc_s.at[0], misc_r.at[0], z_peer)
    z_send_piece(0)
    spike_copy.start()
    tok_z(0)
    z_send_piece(1)
    tok_z(1)
    for i in range(2, OUT + len(out_weights)):
        z_send_piece(i)

    def region(i, src, of_line, side=None):
        if i < OUT:
            span = pl.ds(pl.multiple_of(src * depth + of_line * piece, piece), piece)
            lanes = slice(None) if side is None else pl.ds(side * (wide // 2), wide // 2)
            return w_all.at[i, span, lanes]
        which = slice(None) if side is None else pl.ds(side, 1)
        return wo_all.at[which, aligned(of_line, out_piece), aligned(src, shard)]

    x_copies, y_copies, a_copies, b_copies = {}, {}, {}, {}

    def source(j):
        return lax.rem(s + ring - j, ring)

    def first_stage(i):
        for j in z_span:
            for k in [i] if i < OUT else [OUT, OUT + 1]:
                z_copies[k, j].wait_recv()
            block = region(i, source(j), line)
            for a in x_span:
                x_copies[i, j, a] = copy(block, block, x_send.at[i, j - 1, a - 1], x_recv.at[i, j - 1, a - 1], x_at(a))
                x_copies[i, j, a].start()
            for c in y_span:
                y_copies[i, j, c] = copy(block, block, y_send.at[i, j - 1, c - 1], y_recv.at[i, j - 1, c - 1], y_at(c))
                y_copies[i, j, c].start()

    def second_stage(i):
        for j in z_span:
            for a in x_span:
                x_copies[i, j, a].wait_recv()
                behind = g * across + lax.rem(f + across - a, across)
                block = region(i, source(j), behind, 0)
                for c in y_span:
                    one = copy(block, block, a_send.at[i, j - 1, a - 1, c - 1], a_recv.at[i, j - 1, a - 1, c - 1], y_at(c))
                    one.start()
                    a_copies[i, j, a, c] = one
            for c in y_span:
                y_copies[i, j, c].wait_recv()
                behind = lax.rem(g + down - c, down) * across + f
                block = region(i, source(j), behind, 1)
                for a in x_span:
                    one = copy(block, block, b_send.at[i, j - 1, a - 1, c - 1], b_recv.at[i, j - 1, a - 1, c - 1], x_at(a))
                    one.start()
                    b_copies[i, j, a, c] = one

    def drain(i):
        for j in z_span:
            for a in x_span:
                for c in y_span:
                    a_copies[i, j, a, c].wait_recv()
                    b_copies[i, j, a, c].wait_recv()
        if i < OUT:
            local[2 + i].wait()

    def normalise(side):
        step = 32

        @pl.loop(0, rows // step)
        def _(r):
            block = tok_all[side, aligned(r, step), :].astype(F32)
            scale = lax.rsqrt(jnp.mean(block * block, axis=-1, keepdims=True) + EPS)
            span = pl.ds(pl.multiple_of(side * rows + r * step, step), step)
            normed[span, :] = (block * scale * gain_ref[...]).astype(BF16)

        gates = mm(normed[aligned(side, rows), :], gates_ref[...]).astype(BF16).astype(F32)
        small[:, aligned(side, rows)] = gates.T[: small.shape[0]]

    def project(i):
        @pl.loop(0, 2)
        def _(r):
            span = aligned(r, rows)
            raw[i, span, :] = mm(normed[span, :], w_all[i]).astype(BF16)

    row_id = lax.broadcasted_iota(jnp.int32, (CHUNK, CHUNK), 0)
    col_id = lax.broadcasted_iota(jnp.int32, (CHUNK, CHUNK), 1)
    lower = row_id >= col_id
    strict = row_id > col_id
    eye = jnp.where(row_id == col_id, 1.0, 0.0)

    def decays():
        rows_ref[...] = jnp.zeros_like(rows_ref)
        for h in range(heads):
            head = (2 * t + b) * heads + h
            spike = jnp.concatenate([spikes[side, pl.ds(b * heads + h, 1), :] for side in range(2)], axis=1)
            rate = jnp.exp(jnp.full((1, pos), rate_ref[head], F32))
            rows_ref[h : h + 1, :] = -rate * softplus(small[pl.ds(head, 1), :]) + spike
            level = small[pl.ds(small.shape[0] // 2 + head, 1), :] + bias_ref[head]
            rows_ref[heads + h : heads + h + 1, :] = jax.nn.sigmoid(level)
        upper = jnp.where(row_id <= col_id, 1.0, 0.0)
        decay_row = lax.broadcasted_iota(jnp.int32, (rows_ref.shape[0], CHUNK), 0) < heads
        for c in range(chunks):
            lanes = slice(c * CHUNK, (c + 1) * CHUNK)
            block = rows_ref[:, lanes]
            block = jnp.where(decay_row, mm(block, upper, HIGH), block)
            rows_ref[:, lanes] = block
            cols_ref[lanes, :] = jnp.concatenate([block, jnp.zeros((HEAD - block.shape[0], CHUNK), F32)], axis=0).T

    def unit_of(u):
        return u % heads, slice((u // heads) * CHUNK, (u // heads + 1) * CHUNK)

    def lanes_of(h):
        return slice(h * HEAD, (h + 1) * HEAD)

    def cum_col(u):
        h, span = unit_of(u)
        return cols_ref[span, h : h + 1]

    def beta_col(u):
        h, span = unit_of(u)
        return cols_ref[span, heads + h : heads + h + 1]

    def inverses(units):
        a = []
        for u in units:
            h, span = unit_of(u)
            keys = unit(silu(raw[0, span, lanes_of(h)].astype(F32)))
            diff = cum_col(u) - rows_ref[h : h + 1, span]
            gamma = jnp.where(lower, jnp.exp(jnp.where(lower, diff, 0.0)), 0.0)
            k_all[u] = keys
            gamma_all[u] = gamma
            a.append(jnp.where(strict, mm3(keys * beta_col(u), keys, mm_nt) * gamma, 0.0))
        size = 1
        inv = None
        while size < CHUNK:
            pair = 2 * size
            off = (row_id // pair == col_id // pair) & (row_id % pair >= size) & (col_id % pair < size)
            cross = [jnp.where(off, x, 0.0) for x in a]
            if inv is None:
                inv = [eye - x for x in cross]
            else:
                mid = [mm3(x, y) for x, y in zip(cross, inv)]
                inv = [y - mm3(y, x) for x, y in zip(mid, inv)]
            size = pair
        for u, x in zip(units, inv):
            t_all[u] = x

    def blocks(units):
        for u in units:
            h, span = unit_of(u)
            keys = k_all[u]
            query = unit(silu(raw[1, span, lanes_of(h)].astype(F32))) * HEAD ** (-0.5)
            values = silu(raw[2, span, lanes_of(h)].astype(F32))
            cum = cum_col(u)
            beta = beta_col(u)
            grow = jnp.exp(cum)
            last = cum[CHUNK - 1 :, :]
            right = jnp.concatenate([values * beta, keys * beta * grow], axis=1)
            solved = mm3(t_all[u], right)
            q_k = mm1(query, keys, mm_nt) * gamma_all[u]
            inner = mm1(q_k, solved)
            p_all[u] = query * grow - inner[:, HEAD:]
            u_all[u] = inner[:, :HEAD]
            state = mm3(keys * jnp.exp(last - cum), solved, mm_tn)
            m_all[u] = eye * jnp.exp(last) - state[:, HEAD:]
            o_all[u] = state[:, :HEAD]

    def recurrence():
        for h in range(heads):
            p_out[h, :CHUNK, :] = p_all[h]
            u_out[h, :CHUNK, :] = u_all[h]
        x = [jnp.concatenate([o_all[h], m_all[h]], axis=1) for h in range(heads)]
        for c in range(1, chunks):
            span = slice(c * CHUNK, (c + 1) * CHUNK)
            for h in range(heads):
                u = c * heads + h
                out = mm1(p_all[u], x[h])
                u_out[h, span, :] = out[:, :HEAD] + u_all[u]
                p_out[h, span, :] = out[:, HEAD:]
                nxt = mm3(m_all[u], x[h])
                x[h] = jnp.concatenate([nxt[:, :HEAD] + o_all[u], nxt[:, HEAD:]], axis=1)
        for h in range(heads):
            x_end[h] = x[h]

    state_copy = copy(st_send, st_recv, misc_s.at[1], misc_r.at[1], ahead)

    def send_state():
        @pl.when(s + 2 < ring)
        def _():
            for h in range(heads):
                st_send[h] = (x_end[h, :, :HEAD] + mm3(x_end[h, :, HEAD:], st_first[h])).astype(BF16)
            state_copy.start()

    rim_copy = copy(tail, rim, misc_s.at[2], misc_r.at[2], ahead)

    def gated():
        @pl.loop(0, pos // CHUNK)
        def _(r):
            span = aligned(r, CHUNK)
            glu = raw[3, span, :].astype(F32) * jax.nn.sigmoid(raw[4, span, :].astype(F32))
            ext[pl.ds(pl.multiple_of(pad + r * CHUNK, pad), CHUNK), :] = glu.astype(BF16).astype(F32)

        @pl.when(s + 2 < ring)
        def _():
            tail[...] = ext[pos:, :].astype(BF16)
            rim_copy.start()

    my_chan = pl.ds(pl.multiple_of((2 * t + b) * wide, wide), wide)
    step = 64
    lane = lax.broadcasted_iota(jnp.int32, (step, HEAD), 1)

    def convolve(r):
        acc = jnp.zeros((step, wide), F32)
        window = ext[pl.ds(pl.multiple_of(r * step, step), step + pad), :]
        first = pad - tap_count + 1
        for phase in range(8):
            offsets = [o for o in range(first, first + tap_count) if o % 8 == phase]
            shifted = window[phase : offsets[-1] + step]
            for o in offsets:
                tap = taps_ref[o - first : o - first + 1, my_chan]
                acc = acc + tap * shifted[o - phase : o - phase + step]
        conv_ref[aligned(r, step), :] = acc
        total = jnp.sum(acc, axis=-1, keepdims=True)
        squares = jnp.sum(acc * acc, axis=-1, keepdims=True)
        stat_ref[aligned(r, step), :] = jnp.where(lane == 0, total, jnp.where(lane == 1, squares, 0.0))

    local[0].wait()
    to_partner.wait_recv()
    normalise(b)
    first_stage(0)
    forwards = []

    def forward_tok(h):
        toks[h].wait_recv()
        block = tok_place(1 - b, h, t)
        one = copy(block, block, tok_sem_s.at[2 + h], tok_sem_r.at[2 + h], partner)
        one.start()
        forwards.append(one)

    forward_tok(0)
    first_stage(1)
    second_stage(0)
    forward_tok(1)
    first_stage(2)
    second_stage(1)
    for one in forwards:
        one.wait_recv()
    local[1].wait()
    spike_copy.wait_recv()
    normalise(1 - b)
    decays()
    drain(0)
    project(0)
    units = list(range(chunks * heads))
    group = 2 * heads
    inverses(units[:group])
    first_stage(3)
    second_stage(2)
    inverses(units[group:])
    drain(1)
    project(1)
    first_stage(4)
    second_stage(3)
    drain(2)
    project(2)
    blocks(units)
    second_stage(4)
    first_stage(OUT)
    recurrence()

    @pl.when(s < 2)
    def _():
        for h in range(heads):
            st_first[h] = state_ref[b * heads + h]
        send_state()

    drain(3)
    project(3)
    drain(4)
    project(4)
    second_stage(OUT)
    gated()

    @pl.loop(1, pos // step)
    def _(r):
        convolve(r)

    @pl.when(s < 2)
    def _():
        ext[:pad, :] = jnp.zeros((pad, wide), F32)

    @pl.when(s >= 2)
    def _():
        rim_copy.wait_recv()
        ext[:pad, :] = rim[...].astype(F32)

    convolve(0)
    sums[0] = stat_ref[...].T[: sums.shape[1]]
    sum_copies = [
        copy(sums.at[0], sums.at[1 + d], sum_s.at[d], sum_r.at[d], peer)
        for d, peer in enumerate((partner, z_peer, far))
    ]
    for one in sum_copies:
        one.start()

    @pl.when(s >= 2)
    def _():
        state_copy.wait_recv()
        for h in range(heads):
            st_first[h] = st_recv[h].astype(F32)
        send_state()

    for h in range(heads):
        attn = mm1(p_out[h], st_first[h]) + u_out[h]
        attn = attn * lax.rsqrt(jnp.mean(attn * attn, axis=-1, keepdims=True) + EPS) * head_gain_ref[...]
        mix[:, lanes_of(h)] = attn.astype(BF16)

    for one in sum_copies:
        one.wait_recv()
    total = sums[0] + sums[1] + sums[2] + sums[3]
    mean = total[0:1] / channels
    scale = lax.rsqrt(total[1:2] / channels - mean * mean + EPS)
    stats = jnp.concatenate([mean, scale, jnp.zeros((HEAD - 2, pos), F32)], axis=0)
    stat_ref[...] = stats.T

    @pl.loop(0, pos // step)
    def _(r):
        span = aligned(r, step)
        stat = stat_ref[span, :]
        value = (conv_ref[span, :] - stat[:, 0:1]) * stat[:, 1:2] * chan_gain_ref[:, my_chan]
        mix[span, wide:] = silu(value).astype(BF16)

    drain(OUT)
    for one in local[2 + OUT :]:
        one.wait()
    width = to_z.shape[2]
    parts = half // width

    def product(side, c, of_tp):
        block = mix[aligned(side, rows), :]
        lanes = pl.ds(pl.multiple_of(of_tp * half + c * width, width), width)
        return mm(block[:, :wide], wo_all[0, :, lanes]) + mm(block[:, wide:], wo_all[1, :, lanes])

    order = [(p, c) for p in range(2) for c in range(parts)]
    pairs, z_outs = {}, {}

    def give(p, c):
        to_pair[p, c] = product(1 - b if p == 0 else b, c, 1 - t).astype(BF16)
        one = copy(to_pair.at[p, c], from_pair.at[p, c], pair_s.at[p, c], pair_r.at[p, c], partner)
        one.start()
        pairs[p, c] = one

    give(*order[0])
    for at, (p, c) in enumerate(order):
        if at + 1 < len(order):
            give(*order[at + 1])
        mine = product(1 - b if p == 0 else b, c, t)
        pairs[p, c].wait_recv()
        mine = mine + from_pair[p, c].astype(F32)
        if p == 0:
            to_z[c] = mine.astype(BF16)
            one = copy(to_z.at[c], from_z.at[c], zo_s.at[c], zo_r.at[c], z_peer)
            one.start()
            z_outs[c] = one
        else:
            own_sum[c] = mine
    for c in range(parts):
        z_outs[c].wait_recv()
        out_ref[:, c * width : (c + 1) * width] = (own_sum[c] + from_z[c].astype(F32)).astype(BF16)

    for group_of in (z_copies, x_copies, y_copies, a_copies, b_copies, toks, pairs, z_outs):
        for one in group_of.values():
            one.wait_send()
    for one in [to_partner, spike_copy] + forwards + sum_copies:
        one.wait_send()

    @pl.when(s + 2 < ring)
    def _():
        state_copy.wait_send()
        rim_copy.wait_send()


def layer(sizes, tokens, weights, outs, spikes, states, gates, gain, rate, bias, head_gain, taps, chan_gain):
    across, ring, down = sizes
    rows, half = tokens.shape
    depth, wide_tp = weights[0].shape
    wide = wide_tp // 2
    heads = wide // HEAD
    pos = 2 * rows
    chunks = pos // CHUNK
    units = chunks * heads
    total = 2 * half
    pad = -(-(taps.shape[0] - 1) // 32) * 32
    width = min(256, half)
    parts = half // width
    dma = pltpu.SemaphoreType.DMA
    vmem = pl.BlockSpec(memory_space=pltpu.VMEM)
    smem = pl.BlockSpec(memory_space=pltpu.SMEM)
    anywhere = pl.BlockSpec(memory_space=pl.ANY)
    scratch = pltpu.VMEM
    square = (units, CHUNK, HEAD)
    pieces, spread = 7, 6
    hops, x_hops, y_hops = (max(size - 1, 1) for size in (ring, across, down))
    return pl.pallas_call(
        functools.partial(layer_kernel, sizes),
        out_shape=jax.ShapeDtypeStruct((rows, half), BF16),
        in_specs=[anywhere] * 8 + [vmem] * 4 + [smem] * 2 + [vmem] * 3,
        out_specs=vmem,
        scratch_shapes=[
            scratch((2, rows, total), BF16),
            scratch((pos, total), BF16),
            scratch((5, depth * ring, wide), BF16),
            scratch((2, wide, total), BF16),
            scratch((5, pos, wide), BF16),
            scratch((2,) + spikes.shape, F32),
            scratch((gates.shape[1] // 8, pos), F32),
            scratch((8, pos), F32),
            scratch((pos, HEAD), F32),
            scratch((units, CHUNK, CHUNK), F32),
            scratch(square, F32),
            scratch((units, CHUNK, CHUNK), F32),
            scratch(square, F32),
            scratch(square, F32),
            scratch((units, HEAD, HEAD), F32),
            scratch((units, HEAD, HEAD), F32),
            scratch((heads, pos, HEAD), F32),
            scratch((heads, pos, HEAD), F32),
            scratch((heads, HEAD, 2 * HEAD), F32),
            scratch((heads, HEAD, HEAD), F32),
            scratch((heads, HEAD, HEAD), BF16),
            scratch((heads, HEAD, HEAD), BF16),
            scratch((pad + pos, wide), F32),
            scratch((pad, wide), BF16),
            scratch((pad, wide), BF16),
            scratch((pos, wide), F32),
            scratch((pos, HEAD), F32),
            scratch((4, 8, pos), F32),
            scratch((pos, 2 * wide), BF16),
            scratch((2, parts, rows, width), BF16),
            scratch((2, parts, rows, width), BF16),
            scratch((parts, rows, width), BF16),
            scratch((parts, rows, width), BF16),
            scratch((parts, rows, width), F32),
            dma((pieces, hops)), dma((pieces, hops)),
            dma((spread, hops, x_hops)), dma((spread, hops, x_hops)),
            dma((spread, hops, y_hops)), dma((spread, hops, y_hops)),
            dma((spread, hops, x_hops, y_hops)), dma((spread, hops, x_hops, y_hops)),
            dma((spread, hops, x_hops, y_hops)), dma((spread, hops, x_hops, y_hops)),
            dma((5,)), dma((5,)), dma((3,)), dma((3,)), dma((3,)), dma((3,)),
            dma((2, parts)), dma((2, parts)), dma((parts,)), dma((parts,)),
            dma((9,)),
        ],
        compiler_params=pltpu.CompilerParams(
            collective_id=1, has_side_effects=True, vmem_limit_bytes=56 * 1024 * 1024
        ),
        name="layer",
    )(tokens, *weights, *outs, spikes, states, gates, gain, rate, bias, head_gain, taps, chan_gain)


def on_device(
    tokens,
    input_norm_gain,
    query_weight,
    key_weight,
    value_weight,
    decay_gate_weight,
    write_strength_weight,
    up_weight,
    gate_half_weight,
    log_decay_rate,
    write_strength_bias,
    decay_spike_added,
    starting_state,
    head_norm_gain,
    convolution_kernel,
    channel_norm_gain,
    delta_output_rows,
    convolution_output_rows,
):
    sizes = (lax.axis_size("fs"), lax.axis_size("sp"), lax.axis_size("grp"))
    heads_tp = decay_spike_added.shape[2]
    heads = decay_gate_weight.shape[1]
    gates = jnp.concatenate([decay_gate_weight, write_strength_weight], axis=1)
    gates = jnp.pad(gates, ((0, 0), (0, 128 - 2 * heads)))
    spikes = jnp.pad(decay_spike_added[0].T, ((0, -heads_tp % 8), (0, 0)))
    return layer(
        sizes,
        tokens[0],
        (query_weight, key_weight, value_weight, up_weight, gate_half_weight),
        (delta_output_rows, convolution_output_rows),
        spikes,
        starting_state[0],
        gates,
        input_norm_gain[None],
        log_decay_rate,
        write_strength_bias,
        head_norm_gain[None],
        convolution_kernel,
        channel_norm_gain[None],
    )[None]


def solution(mesh):
    return jax.shard_map(
        on_device,
        mesh=mesh,
        in_specs=(
            P(("grp", "fs"), "sp", "tp"),
            P(),
            P("sp", "tp"),
            P("sp", "tp"),
            P("sp", "tp"),
            P(),
            P(),
            P("sp", "tp"),
            P("sp", "tp"),
            P(),
            P(),
            P(("grp", "fs"), "sp", "tp"),
            P(("grp", "fs"), "tp", None, None),
            P(),
            P(),
            P(),
            P("tp", "sp"),
            P("tp", "sp"),
        ),
        out_specs=P(("grp", "fs"), "sp", "tp"),
        check_vma=False,
    )
```

```python
import functools

import jax
import jax.numpy as jnp
from jax import lax
from jax.experimental import pallas as pl
from jax.experimental.pallas import tpu as pltpu
from jax.sharding import PartitionSpec as P

HEAD = 128
CHUNK = 128
EPS = 1e-06
HIGH = lax.Precision.HIGHEST
MESH = pl.DeviceIdType.MESH
F32 = jnp.float32
BF16 = jnp.bfloat16


def dot(a, b, dims, precision=None):
    return lax.dot_general(a, b, (dims, ((), ())), preferred_element_type=F32, precision=precision)


def mm(a, b, precision=None):
    return dot(a, b, ((1,), (0,)), precision)


def mm_nt(a, b, precision=None):
    return dot(a, b, ((1,), (1,)), precision)


def mm_tn(a, b, precision=None):
    return dot(a, b, ((0,), (0,)), precision)


def split(x):
    high = x.astype(BF16)
    return high, (x - high.astype(F32)).astype(BF16)


def mm3(a, b, form=mm):
    a_high, a_low = split(a)
    b_high, b_low = split(b)
    return form(a_high, b_high) + (form(a_high, b_low) + form(a_low, b_high))


def mm1(a, b, form=mm):
    return form(a.astype(BF16), b.astype(BF16))


def silu(x):
    return x * jax.nn.sigmoid(x)


def unit(x):
    return x * lax.rsqrt(jnp.sum(x * x, axis=-1, keepdims=True) + EPS)


def softplus(x):
    return jnp.maximum(x, 0.0) + jnp.log1p(jnp.exp(-jnp.abs(x)))


def row_of(block, row):
    here = lax.broadcasted_iota(jnp.int32, block.shape, 0) == row
    return jnp.sum(jnp.where(here, block, 0.0), axis=0, keepdims=True)


def aligned(index, size):
    return pl.ds(pl.multiple_of(index * size, size), size)


def layer_kernel(
    sizes,
    tok_ref, wq_ref, wk_ref, wv_ref, wu_ref, wg_ref, wd_ref, wc_ref,
    spike_ref, state_ref, decay_ref, write_ref, gain_ref, rate_ref, bias_ref, head_gain_ref, taps_ref, chan_gain_ref,
    out_ref,
    tok_all, normed, w_all, wo_all, raw, spikes, small, rows_ref, cols_ref,
    t_all, k_all, gamma_all, p_all, u_all, m_all, o_all, p_out, u_out, x_end,
    st_first, st_send, st_recv, ext, tail, rim, conv_ref, stat_ref, sums, mix,
    to_pair, from_pair, to_z, from_z, own_sum,
    z_send, z_recv, x_send, x_recv, y_send, y_recv, a_send, a_recv, b_send, b_recv,
    tok_sem_s, tok_sem_r, misc_s, misc_r, sum_s, sum_r, pair_s, pair_r, zo_s, zo_r, local_sem,
):
    across, ring, down = sizes
    rows, half = tok_ref.shape
    depth, wide_tp = wq_ref.shape
    wide = wide_tp // 2
    heads = wide // HEAD
    pos = 2 * rows
    chunks = pos // CHUNK
    shard = wd_ref.shape[1]
    lines = down * across
    piece = depth // lines
    out_piece = wide // lines
    tap_count = taps_ref.shape[0]
    channels = taps_ref.shape[1]
    pad = ext.shape[0] - pos

    g, s, f, t = (lax.axis_index(name) for name in ("grp", "sp", "fs", "tp"))
    b = lax.rem(s, 2)
    line = g * across + f
    z_at = lambda j: {"sp": lax.rem(s + j, ring)}
    x_at = lambda a: {"fs": lax.rem(f + a, across)}
    y_at = lambda c: {"grp": lax.rem(g + c, down)}
    partner = {"tp": 1 - t}
    z_peer = {"sp": s + 1 - 2 * b}
    far = {"sp": s + 1 - 2 * b, "tp": 1 - t}
    ahead = {"sp": lax.rem(s + 2, ring)}
    z_span, x_span, y_span = range(1, ring), range(1, across), range(1, down)

    def copy(src, dst, send_sem, recv_sem, peer):
        return pltpu.make_async_remote_copy(
            src_ref=src, dst_ref=dst, send_sem=send_sem, recv_sem=recv_sem, device_id=peer, device_id_type=MESH
        )

    weights = (wk_ref, wq_ref, wv_ref, wu_ref, wg_ref)
    out_weights = (wd_ref, wc_ref)
    OUT = len(weights)

    local = [pltpu.make_async_copy(tok_ref, tok_all.at[b, :, aligned(t, half)], local_sem.at[0])]
    local.append(pltpu.make_async_copy(spike_ref, spikes.at[b], local_sem.at[1 + OUT + len(out_weights)]))
    for i, w in enumerate(weights):
        local.append(
            pltpu.make_async_copy(w.at[:, aligned(b, wide)], w_all.at[i, aligned(s, depth), :], local_sem.at[1 + i])
        )
    for i, w in enumerate(out_weights):
        local.append(
            pltpu.make_async_copy(w.at[aligned(b, wide), :], wo_all.at[i, :, aligned(s, shard)], local_sem.at[1 + OUT + i])
        )
    for one in local:
        one.start()

    barrier = pltpu.get_barrier_semaphore()
    friends = [z_at(j) for j in z_span] + [x_at(a) for a in x_span] + [y_at(c) for c in y_span] + [partner, far]
    for friend in friends:
        pl.semaphore_signal(barrier, inc=1, device_id=friend, device_id_type=MESH)
    pl.semaphore_wait(barrier, len(friends))

    z_copies = {}

    def z_send_piece(i):
        for j in z_span:
            to = lax.rem(lax.rem(s + j, ring), 2)
            if i < OUT:
                src = weights[i].at[aligned(line, piece), aligned(to, wide)]
                dst = w_all.at[i, pl.ds(pl.multiple_of(s * depth + line * piece, piece), piece), :]
            else:
                begin = pl.multiple_of(to * wide + line * out_piece, out_piece)
                src = out_weights[i - OUT].at[pl.ds(begin, out_piece), :]
                dst = wo_all.at[i - OUT, aligned(line, out_piece), aligned(s, shard)]
            one = copy(src, dst, z_send.at[i, j - 1], z_recv.at[i, j - 1], z_at(j))
            one.start()
            z_copies[i, j] = one

    part = rows // 2
    toks = {}

    def tok_place(side, h, from_tp):
        return tok_all.at[side, pl.ds(h * part, part), aligned(from_tp, half)]

    def tok_z(h):
        toks[h] = copy(
            tok_ref.at[pl.ds(h * part, part), :], tok_place(b, h, t), tok_sem_s.at[h], tok_sem_r.at[h], z_peer
        )
        toks[h].start()

    to_partner = copy(tok_ref, tok_all.at[b, :, aligned(t, half)], tok_sem_s.at[4], tok_sem_r.at[4], partner)
    to_partner.start()
    spike_copy = copy(spike_ref, spikes.at[b], misc_s.at[0], misc_r.at[0], z_peer)
    spike_copy.start()
    for i in range(OUT - 1):
        z_send_piece(i)
    tok_z(0)
    z_send_piece(OUT - 1)
    z_send_piece(OUT)
    tok_z(1)
    z_send_piece(OUT + 1)

    def region(i, src, of_line, side=None):
        if i < OUT:
            span = pl.ds(pl.multiple_of(src * depth + of_line * piece, piece), piece)
            lanes = slice(None) if side is None else pl.ds(side * (wide // 2), wide // 2)
            return w_all.at[i, span, lanes]
        count = out_piece if side is None else out_piece // 2
        begin = of_line * out_piece + (0 if side is None else side * count)
        return wo_all.at[i - OUT, pl.ds(pl.multiple_of(begin, count), count), aligned(src, shard)]

    x_copies, y_copies, a_copies, b_copies = {}, {}, {}, {}

    def source(j):
        return lax.rem(s + ring - j, ring)

    def first_stage(i):
        for j in z_span:
            z_copies[i, j].wait_recv()
            block = region(i, source(j), line)
            for a in x_span:
                x_copies[i, j, a] = copy(block, block, x_send.at[i, j - 1, a - 1], x_recv.at[i, j - 1, a - 1], x_at(a))
                x_copies[i, j, a].start()
            for c in y_span:
                y_copies[i, j, c] = copy(block, block, y_send.at[i, j - 1, c - 1], y_recv.at[i, j - 1, c - 1], y_at(c))
                y_copies[i, j, c].start()

    def second_stage(i):
        for j in z_span:
            for a in x_span:
                x_copies[i, j, a].wait_recv()
                behind = g * across + lax.rem(f + across - a, across)
                block = region(i, source(j), behind, 0)
                for c in y_span:
                    one = copy(block, block, a_send.at[i, j - 1, a - 1, c - 1], a_recv.at[i, j - 1, a - 1, c - 1], y_at(c))
                    one.start()
                    a_copies[i, j, a, c] = one
            for c in y_span:
                y_copies[i, j, c].wait_recv()
                behind = lax.rem(g + down - c, down) * across + f
                block = region(i, source(j), behind, 1)
                for a in x_span:
                    one = copy(block, block, b_send.at[i, j - 1, a - 1, c - 1], b_recv.at[i, j - 1, a - 1, c - 1], x_at(a))
                    one.start()
                    b_copies[i, j, a, c] = one

    def drain(i, hops=z_span):
        for j in hops:
            for a in x_span:
                for c in y_span:
                    a_copies[i, j, a, c].wait_recv()
                    b_copies[i, j, a, c].wait_recv()
        if hops is z_span:
            local[2 + i].wait()

    def rows_at(start, count):
        return pl.ds(pl.multiple_of(start, CHUNK), count)

    def normalise(side, begin, count):
        step = 32

        @pl.loop(0, count // step)
        def _(r):
            block = tok_all[side, pl.ds(pl.multiple_of(begin + r * step, step), step), :].astype(F32)
            scale = lax.rsqrt(jnp.mean(block * block, axis=-1, keepdims=True) + EPS)
            span = pl.ds(pl.multiple_of(side * rows + begin + r * step, step), step)
            normed[span, :] = (block * scale * gain_ref[...]).astype(BF16)

        span = rows_at(side * rows + begin, count)
        block = normed[span, :]
        for w, gate_ref in enumerate((decay_ref, write_ref)):
            small[w, :, span] = mm_nt(gate_ref[...], block).astype(BF16).astype(F32)

    def project(i, start, count):
        span = rows_at(start, count)
        raw[i, span, :] = mm(normed[span, :], w_all[i]).astype(BF16)

    row_id = lax.broadcasted_iota(jnp.int32, (CHUNK, CHUNK), 0)
    col_id = lax.broadcasted_iota(jnp.int32, (CHUNK, CHUNK), 1)
    lower = row_id >= col_id
    strict = row_id > col_id
    eye = jnp.where(row_id == col_id, 1.0, 0.0)

    rows_ref[...] = jnp.zeros_like(rows_ref)

    def decays(side, begin, count):
        span = rows_at(side * rows + begin, count)
        for h in range(heads):
            head = (2 * t + b) * heads + h
            rate = jnp.exp(jnp.full((1, count), rate_ref[head], F32))
            spike = row_of(spikes[side, :, begin : begin + count], b * heads + h)
            rows_ref[h : h + 1, span] = -rate * softplus(row_of(small[0, :, span], head)) + spike
            level = row_of(small[1, :, span], head) + bias_ref[head]
            rows_ref[heads + h : heads + h + 1, span] = jax.nn.sigmoid(level)
        upper = jnp.where(row_id <= col_id, 1.0, 0.0)
        decay_row = lax.broadcasted_iota(jnp.int32, (rows_ref.shape[0], CHUNK), 0) < heads
        for c in range(count // CHUNK):
            lanes = rows_at(side * rows + begin + c * CHUNK, CHUNK)
            block = rows_ref[:, lanes]
            block = jnp.where(decay_row, mm(block, upper, HIGH), block)
            rows_ref[:, lanes] = block
            cols_ref[lanes, :] = jnp.concatenate([block, jnp.zeros((HEAD - block.shape[0], CHUNK), F32)], axis=0).T

    def units_of(start, count):
        first = start // CHUNK
        return [(h, first + c) for c in range(count // CHUNK) for h in range(heads)]

    def unit_of(u):
        return u[0], aligned(u[1], CHUNK)

    def slot(u):
        return u[1] * heads + u[0]

    def lanes_of(h):
        return slice(h * HEAD, (h + 1) * HEAD)

    def cum_col(u):
        h, span = unit_of(u)
        return cols_ref[span, h : h + 1]

    def beta_col(u):
        h, span = unit_of(u)
        return cols_ref[span, heads + h : heads + h + 1]

    def inverses(start, count):
        units = units_of(start, count)
        a = []
        for u in units:
            h, span = unit_of(u)
            keys = unit(silu(raw[0, span, lanes_of(h)].astype(F32)))
            diff = cum_col(u) - rows_ref[h : h + 1, span]
            gamma = jnp.where(lower, jnp.exp(jnp.where(lower, diff, 0.0)), 0.0)
            k_all[slot(u)] = keys
            gamma_all[slot(u)] = gamma
            a.append(jnp.where(strict, mm3(keys * beta_col(u), keys, mm_nt) * gamma, 0.0))
        size = 1
        inv = None
        while size < CHUNK:
            pair = 2 * size
            off = (row_id // pair == col_id // pair) & (row_id % pair >= size) & (col_id % pair < size)
            cross = [jnp.where(off, x, 0.0) for x in a]
            if inv is None:
                inv = [eye - x for x in cross]
            else:
                mid = [mm3(x, y) for x, y in zip(cross, inv)]
                inv = [y - mm3(y, x) for x, y in zip(mid, inv)]
            size = pair
        for u, x in zip(units, inv):
            t_all[slot(u)] = x

    def blocks(start, count):
        for u in units_of(start, count):
            h, span = unit_of(u)
            keys = k_all[slot(u)]
            query = unit(silu(raw[1, span, lanes_of(h)].astype(F32))) * HEAD ** (-0.5)
            values = silu(raw[2, span, lanes_of(h)].astype(F32))
            cum = cum_col(u)
            beta = beta_col(u)
            grow = jnp.exp(cum)
            last = cum[CHUNK - 1 :, :]
            right = jnp.concatenate([values * beta, keys * beta * grow], axis=1)
            solved = mm3(t_all[slot(u)], right)
            q_k = mm1(query, keys, mm_nt) * gamma_all[slot(u)]
            inner = mm1(q_k, solved)
            p_all[slot(u)] = query * grow - inner[:, HEAD:]
            u_all[slot(u)] = inner[:, :HEAD]
            state = mm3(keys * jnp.exp(last - cum), solved, mm_tn)
            m_all[slot(u)] = eye * jnp.exp(last) - state[:, HEAD:]
            o_all[slot(u)] = state[:, :HEAD]

    def recurrence():
        for h in range(heads):
            p_out[h, :CHUNK, :] = p_all[h]
            u_out[h, :CHUNK, :] = u_all[h]
        x = [jnp.concatenate([o_all[h], m_all[h]], axis=1) for h in range(heads)]
        for c in range(1, chunks):
            span = slice(c * CHUNK, (c + 1) * CHUNK)
            for h in range(heads):
                u = c * heads + h
                out = mm1(p_all[u], x[h])
                u_out[h, span, :] = out[:, :HEAD] + u_all[u]
                p_out[h, span, :] = out[:, HEAD:]
                nxt = mm3(m_all[u], x[h])
                x[h] = jnp.concatenate([nxt[:, :HEAD] + o_all[u], nxt[:, HEAD:]], axis=1)
        for h in range(heads):
            x_end[h] = x[h]

    state_copy = copy(st_send, st_recv, misc_s.at[1], misc_r.at[1], ahead)

    def send_state():
        @pl.when(s + 2 < ring)
        def _():
            for h in range(heads):
                st_send[h] = (x_end[h, :, :HEAD] + mm3(x_end[h, :, HEAD:], st_first[h])).astype(BF16)
            state_copy.start()

    rim_copy = copy(tail, rim, misc_s.at[2], misc_r.at[2], ahead)

    def gated():
        @pl.loop(0, pos // CHUNK)
        def _(r):
            span = aligned(r, CHUNK)
            glu = raw[3, span, :].astype(F32) * jax.nn.sigmoid(raw[4, span, :].astype(F32))
            ext[pl.ds(pl.multiple_of(pad + r * CHUNK, pad), CHUNK), :] = glu.astype(BF16).astype(F32)

        @pl.when(s + 2 < ring)
        def _():
            tail[...] = ext[pos:, :].astype(BF16)
            rim_copy.start()

    my_chan = pl.ds(pl.multiple_of((2 * t + b) * wide, wide), wide)
    step = 64
    lane = lax.broadcasted_iota(jnp.int32, (step, HEAD), 1)

    def convolve(r):
        acc = jnp.zeros((step, wide), F32)
        window = ext[pl.ds(pl.multiple_of(r * step, step), step + pad), :]
        first = pad - tap_count + 1
        for phase in range(8):
            offsets = [o for o in range(first, first + tap_count) if o % 8 == phase]
            shifted = window[phase : offsets[-1] + step]
            for o in offsets:
                tap = taps_ref[o - first : o - first + 1, my_chan]
                acc = acc + tap * shifted[o - phase : o - phase + step]
        conv_ref[aligned(r, step), :] = acc
        total = jnp.sum(acc, axis=-1, keepdims=True)
        squares = jnp.sum(acc * acc, axis=-1, keepdims=True)
        stat_ref[aligned(r, step), :] = jnp.where(lane == 0, total, jnp.where(lane == 1, squares, 0.0))

    mine = b * rows
    peers = (1 - b) * rows
    peers_late = peers + part
    forwards = []

    def forward_tok(h):
        toks[h].wait_recv()
        block = tok_place(1 - b, h, t)
        one = copy(block, block, tok_sem_s.at[2 + h], tok_sem_r.at[2 + h], partner)
        one.start()
        forwards.append(one)

    local[0].wait()
    local[1].wait()
    to_partner.wait_recv()
    normalise(b, 0, rows)
    decays(b, 0, rows)
    first_stage(0)
    first_stage(1)
    second_stage(0)
    first_stage(2)
    second_stage(1)
    first_stage(3)
    drain(0)
    project(0, mine, rows)
    inverses(mine, rows)
    second_stage(2)
    forward_tok(0)
    drain(1)
    project(1, mine, rows)
    spike_copy.wait_recv()
    forwards[0].wait_recv()
    normalise(1 - b, 0, part)
    decays(1 - b, 0, part)
    first_stage(4)
    second_stage(3)
    drain(2)
    project(2, mine, rows)
    blocks(mine, rows)
    first_stage(OUT)
    for i in range(3):
        project(i, peers, part)
    inverses(peers, part)
    second_stage(4)
    drain(3)
    project(3, mine, rows)
    project(3, peers, part)
    forward_tok(1)
    blocks(peers, part)
    forwards[1].wait_recv()
    normalise(1 - b, part, part)
    decays(1 - b, part, part)
    second_stage(OUT)
    for i in range(4):
        project(i, peers_late, part)
    drain(4)
    project(4, mine, rows)
    project(4, peers, rows)
    first_stage(OUT + 1)
    gated()
    inverses(peers_late, part)
    blocks(peers_late, part)
    recurrence()

    @pl.when(s < 2)
    def _():
        for h in range(heads):
            st_first[h] = state_ref[b * heads + h]
        send_state()

    @pl.loop(1, pos // step)
    def _(r):
        convolve(r)

    second_stage(OUT + 1)

    @pl.when(s < 2)
    def _():
        ext[:pad, :] = jnp.zeros((pad, wide), F32)

    @pl.when(s >= 2)
    def _():
        rim_copy.wait_recv()
        ext[:pad, :] = rim[...].astype(F32)

    convolve(0)
    sums[0] = stat_ref[...].T[: sums.shape[1]]
    sum_copies = [
        copy(sums.at[0], sums.at[1 + d], sum_s.at[d], sum_r.at[d], peer)
        for d, peer in enumerate((partner, z_peer, far))
    ]
    for one in sum_copies:
        one.start()

    @pl.when(s >= 2)
    def _():
        state_copy.wait_recv()
        for h in range(heads):
            st_first[h] = st_recv[h].astype(F32)
        send_state()

    for h in range(heads):
        attn = mm1(p_out[h], st_first[h]) + u_out[h]
        attn = attn * lax.rsqrt(jnp.mean(attn * attn, axis=-1, keepdims=True) + EPS) * head_gain_ref[...]
        mix[:, lanes_of(h)] = attn.astype(BF16)

    for one in sum_copies:
        one.wait_recv()
    total = sums[0] + sums[1] + sums[2] + sums[3]
    mean = total[0:1] / channels
    scale = lax.rsqrt(total[1:2] / channels - mean * mean + EPS)
    stats = jnp.concatenate([mean, scale, jnp.zeros((HEAD - 2, pos), F32)], axis=0)
    stat_ref[...] = stats.T

    @pl.loop(0, pos // step)
    def _(r):
        span = aligned(r, step)
        stat = stat_ref[span, :]
        value = (conv_ref[span, :] - stat[:, 0:1]) * stat[:, 1:2] * chan_gain_ref[:, my_chan]
        mix[span, wide:] = silu(value).astype(BF16)

    for one in local[2 + OUT :]:
        one.wait()
    turns = ring // 2
    width = to_z.shape[2]
    parts = shard // width

    def product(side, lane, of_tp):
        block = mix[aligned(side, rows), :]
        lanes = pl.ds(pl.multiple_of(of_tp * half + lane, width), width)
        return mm(block[:, :wide], wo_all[0, :, lanes]) + mm(block[:, wide:], wo_all[1, :, lanes])

    order = [(k, p, c) for k in range(turns) for p in range(2) for c in range(parts)]
    pairs = {}

    def place(k, c):
        return lax.rem(lax.rem(s, turns) + k, turns) * parts + c

    def give(k, p, c):
        if p == 0 and c == 0:
            for j in ((turns - k) % turns, (turns - k) % turns + turns):
                if j:
                    drain(OUT, (j,))
                    drain(OUT + 1, (j,))
        at = k * parts + c
        to_pair[p, at] = product(1 - b if p == 0 else b, place(k, c) * width, 1 - t).astype(BF16)
        one = copy(to_pair.at[p, at], from_pair.at[p, at], pair_s.at[p, at], pair_r.at[p, at], partner)
        one.start()
        pairs[k, p, c] = one

    def slot_copy(at):
        return copy(to_z.at[at], from_z.at[at], zo_s.at[at], zo_r.at[at], z_peer)

    give(*order[0])
    for at, (k, p, c) in enumerate(order):
        if at + 1 < len(order):
            give(*order[at + 1])
        mine = product(1 - b if p == 0 else b, place(k, c) * width, t)
        pairs[k, p, c].wait_recv()
        mine = mine + from_pair[p, k * parts + c].astype(F32)
        if p == 0:
            to_z[place(k, c)] = mine.astype(BF16)
            slot_copy(place(k, c)).start()
        else:
            own_sum[place(k, c)] = mine
    for at in range(turns * parts):
        slot_copy(at).wait_recv()
        out_ref[:, at * width : (at + 1) * width] = (own_sum[at] + from_z[at].astype(F32)).astype(BF16)
        slot_copy(at).wait_send()

    for group_of in (z_copies, x_copies, y_copies, a_copies, b_copies, toks, pairs):
        for one in group_of.values():
            one.wait_send()
    for one in [to_partner, spike_copy] + forwards + sum_copies:
        one.wait_send()

    @pl.when(s + 2 < ring)
    def _():
        state_copy.wait_send()
        rim_copy.wait_send()


def layer(sizes, tokens, weights, outs, spikes, states, decay_gates, write_gates, gain, rate, bias, head_gain, taps, chan_gain):
    across, ring, down = sizes
    rows, half = tokens.shape
    depth, wide_tp = weights[0].shape
    wide = wide_tp // 2
    heads = wide // HEAD
    pos = 2 * rows
    chunks = pos // CHUNK
    units = chunks * heads
    total = 2 * half
    pad = -(-(taps.shape[0] - 1) // 32) * 32
    width = min(256, outs[0].shape[1])
    parts = half // width
    dma = pltpu.SemaphoreType.DMA
    vmem = pl.BlockSpec(memory_space=pltpu.VMEM)
    smem = pl.BlockSpec(memory_space=pltpu.SMEM)
    anywhere = pl.BlockSpec(memory_space=pl.ANY)
    scratch = pltpu.VMEM
    square = (units, CHUNK, HEAD)
    pieces = spread = 7
    hops, x_hops, y_hops = (max(size - 1, 1) for size in (ring, across, down))
    return pl.pallas_call(
        functools.partial(layer_kernel, sizes),
        out_shape=jax.ShapeDtypeStruct((rows, half), BF16),
        in_specs=[anywhere] * 8 + [vmem] * 5 + [smem] * 2 + [vmem] * 3,
        out_specs=vmem,
        scratch_shapes=[
            scratch((2, rows, total), BF16),
            scratch((pos, total), BF16),
            scratch((5, depth * ring, wide), BF16),
            scratch((2, wide, total), BF16),
            scratch((5, pos, wide), BF16),
            scratch((2,) + spikes.shape, F32),
            scratch((2, decay_gates.shape[0], pos), F32),
            scratch((8, pos), F32),
            scratch((pos, HEAD), F32),
            scratch((units, CHUNK, CHUNK), F32),
            scratch(square, F32),
            scratch((units, CHUNK, CHUNK), F32),
            scratch(square, F32),
            scratch(square, F32),
            scratch((units, HEAD, HEAD), F32),
            scratch((units, HEAD, HEAD), F32),
            scratch((heads, pos, HEAD), F32),
            scratch((heads, pos, HEAD), F32),
            scratch((heads, HEAD, 2 * HEAD), F32),
            scratch((heads, HEAD, HEAD), F32),
            scratch((heads, HEAD, HEAD), BF16),
            scratch((heads, HEAD, HEAD), BF16),
            scratch((pad + pos, wide), F32),
            scratch((pad, wide), BF16),
            scratch((pad, wide), BF16),
            scratch((pos, wide), F32),
            scratch((pos, HEAD), F32),
            scratch((4, 8, pos), F32),
            scratch((pos, 2 * wide), BF16),
            scratch((2, parts, rows, width), BF16),
            scratch((2, parts, rows, width), BF16),
            scratch((parts, rows, width), BF16),
            scratch((parts, rows, width), BF16),
            scratch((parts, rows, width), F32),
            dma((pieces, hops)), dma((pieces, hops)),
            dma((spread, hops, x_hops)), dma((spread, hops, x_hops)),
            dma((spread, hops, y_hops)), dma((spread, hops, y_hops)),
            dma((spread, hops, x_hops, y_hops)), dma((spread, hops, x_hops, y_hops)),
            dma((spread, hops, x_hops, y_hops)), dma((spread, hops, x_hops, y_hops)),
            dma((5,)), dma((5,)), dma((3,)), dma((3,)), dma((3,)), dma((3,)),
            dma((2, parts)), dma((2, parts)), dma((parts,)), dma((parts,)),
            dma((9,)),
        ],
        compiler_params=pltpu.CompilerParams(
            collective_id=1, has_side_effects=True, vmem_limit_bytes=56 * 1024 * 1024
        ),
        name="layer",
    )(tokens, *weights, *outs, spikes, states, decay_gates, write_gates, gain, rate, bias, head_gain, taps, chan_gain)


def on_device(
    tokens,
    input_norm_gain,
    query_weight,
    key_weight,
    value_weight,
    decay_gate_weight,
    write_strength_weight,
    up_weight,
    gate_half_weight,
    log_decay_rate,
    write_strength_bias,
    decay_spike_added,
    starting_state,
    head_norm_gain,
    convolution_kernel,
    channel_norm_gain,
    delta_output_rows,
    convolution_output_rows,
):
    sizes = (lax.axis_size("fs"), lax.axis_size("sp"), lax.axis_size("grp"))
    return layer(
        sizes,
        tokens[0],
        (query_weight, key_weight, value_weight, up_weight, gate_half_weight),
        (delta_output_rows, convolution_output_rows),
        decay_spike_added[0].T,
        starting_state[0],
        decay_gate_weight.T,
        write_strength_weight.T,
        input_norm_gain[None],
        log_decay_rate,
        write_strength_bias,
        head_norm_gain[None],
        convolution_kernel,
        channel_norm_gain[None],
    )[None]


def solution(mesh):
    return jax.shard_map(
        on_device,
        mesh=mesh,
        in_specs=(
            P(("grp", "fs"), "sp", "tp"),
            P(),
            P("sp", "tp"),
            P("sp", "tp"),
            P("sp", "tp"),
            P(),
            P(),
            P("sp", "tp"),
            P("sp", "tp"),
            P(),
            P(),
            P(("grp", "fs"), "sp", "tp"),
            P(("grp", "fs"), "tp", None, None),
            P(),
            P(),
            P(),
            P("tp", "sp"),
            P("tp", "sp"),
        ),
        out_specs=P(("grp", "fs"), "sp", "tp"),
        check_vma=False,
    )
```

```python
import functools

import jax
import jax.numpy as jnp
from jax import lax
from jax.experimental import pallas as pl
from jax.experimental.pallas import tpu as pltpu
from jax.sharding import PartitionSpec as P

HEAD = 128
CHUNK = 128
EPS = 1e-06
HIGH = lax.Precision.HIGHEST
MESH = pl.DeviceIdType.MESH
F32 = jnp.float32
BF16 = jnp.bfloat16


def dot(a, b, dims, precision=None):
    return lax.dot_general(a, b, (dims, ((), ())), preferred_element_type=F32, precision=precision)


def mm(a, b, precision=None):
    return dot(a, b, ((1,), (0,)), precision)


def mm_nt(a, b, precision=None):
    return dot(a, b, ((1,), (1,)), precision)


def mm_tn(a, b, precision=None):
    return dot(a, b, ((0,), (0,)), precision)


def split(x):
    high = x.astype(BF16)
    return high, (x - high.astype(F32)).astype(BF16)


def mm3(a, b, form=mm):
    a_high, a_low = split(a)
    b_high, b_low = split(b)
    return form(a_high, b_high) + (form(a_high, b_low) + form(a_low, b_high))


def mm1(a, b, form=mm):
    return form(a.astype(BF16), b.astype(BF16))


def silu(x):
    return x * jax.nn.sigmoid(x)


def unit(x):
    return x * lax.rsqrt(jnp.sum(x * x, axis=-1, keepdims=True) + EPS)


def softplus(x):
    return jnp.maximum(x, 0.0) + jnp.log1p(jnp.exp(-jnp.abs(x)))


def row_of(block, row):
    here = lax.broadcasted_iota(jnp.int32, block.shape, 0) == row
    return jnp.sum(jnp.where(here, block, 0.0), axis=0, keepdims=True)


def aligned(index, size):
    return pl.ds(pl.multiple_of(index * size, size), size)


def layer_kernel(
    sizes,
    tok_ref, wq_ref, wk_ref, wv_ref, wu_ref, wg_ref, wd_ref, wc_ref,
    spike_ref, state_ref, decay_ref, write_ref, gain_ref, rate_ref, bias_ref, head_gain_ref, taps_ref, chan_gain_ref,
    out_ref,
    tok_all, normed, w_all, wo_all, raw, spikes, small, rows_ref, cols_ref,
    t_all, k_all, gamma_all, p_all, u_all, m_all, o_all, p_out, u_out, x_end,
    st_first, st_send, st_recv, ext, tail, rim, conv_ref, stat_ref, sums, mix,
    to_pair, from_pair, to_z, from_z, own_sum,
    z_send, z_recv, x_send, x_recv, y_send, y_recv, a_send, a_recv, b_send, b_recv,
    tok_sem_s, tok_sem_r, misc_s, misc_r, sum_s, sum_r, pair_s, pair_r, zo_s, zo_r, local_sem,
):
    across, ring, down = sizes
    rows, half = tok_ref.shape
    depth, wide_tp = wq_ref.shape
    wide = wide_tp // 2
    heads = wide // HEAD
    pos = 2 * rows
    chunks = pos // CHUNK
    shard = wd_ref.shape[1]
    lines = down * across
    piece = depth // lines
    out_piece = wide // lines
    tap_count = taps_ref.shape[0]
    channels = taps_ref.shape[1]
    pad = ext.shape[0] - pos

    g, s, f, t = (lax.axis_index(name) for name in ("grp", "sp", "fs", "tp"))
    b = lax.rem(s, 2)
    line = g * across + f
    z_at = lambda j: {"sp": lax.rem(s + j, ring)}
    x_at = lambda a: {"fs": lax.rem(f + a, across)}
    y_at = lambda c: {"grp": lax.rem(g + c, down)}
    partner = {"tp": 1 - t}
    z_peer = {"sp": s + 1 - 2 * b}
    far = {"sp": s + 1 - 2 * b, "tp": 1 - t}
    ahead = {"sp": lax.rem(s + 2, ring)}
    z_span, x_span, y_span = range(1, ring), range(1, across), range(1, down)

    def copy(src, dst, send_sem, recv_sem, peer):
        return pltpu.make_async_remote_copy(
            src_ref=src, dst_ref=dst, send_sem=send_sem, recv_sem=recv_sem, device_id=peer, device_id_type=MESH
        )

    weights = (wk_ref, wq_ref, wv_ref, wu_ref, wg_ref)
    out_weights = (wd_ref, wc_ref)
    OUT = len(weights)
    width = to_z.shape[2]
    splits = shard // width
    turns = half // shard

    def out_lanes(i, src):
        return pl.ds(pl.multiple_of(src * shard + (i - OUT) * width, width), width)


    local = [pltpu.make_async_copy(tok_ref, tok_all.at[b, :, aligned(t, half)], local_sem.at[0])]
    local.append(pltpu.make_async_copy(spike_ref, spikes.at[b], local_sem.at[1 + OUT + len(out_weights)]))
    for i, w in enumerate(weights):
        local.append(
            pltpu.make_async_copy(w.at[:, aligned(b, wide)], w_all.at[i, aligned(s, depth), :], local_sem.at[1 + i])
        )
    for i, w in enumerate(out_weights):
        local.append(
            pltpu.make_async_copy(w.at[aligned(b, wide), :], wo_all.at[i, :, aligned(s, shard)], local_sem.at[1 + OUT + i])
        )
    for one in local:
        one.start()

    barrier = pltpu.get_barrier_semaphore()
    friends = [z_at(j) for j in z_span] + [x_at(a) for a in x_span] + [y_at(c) for c in y_span] + [partner, far]
    for friend in friends:
        pl.semaphore_signal(barrier, inc=1, device_id=friend, device_id_type=MESH)
    pl.semaphore_wait(barrier, len(friends))

    z_copies = {}

    def z_send_piece(i):
        for j in z_span:
            to = lax.rem(lax.rem(s + j, ring), 2)
            if i < OUT:
                src = weights[i].at[aligned(line, piece), aligned(to, wide)]
                dst = w_all.at[i, pl.ds(pl.multiple_of(s * depth + line * piece, piece), piece), :]
                z_copies[i, j] = [copy(src, dst, z_send.at[i, j - 1], z_recv.at[i, j - 1], z_at(j))]
            else:
                begin = pl.multiple_of(to * wide + line * out_piece, out_piece)
                z_copies[i, j] = []
                for half_of, w in enumerate(out_weights):
                    src = w.at[pl.ds(begin, out_piece), pl.ds((i - OUT) * width, width)]
                    dst = wo_all.at[half_of, aligned(line, out_piece), out_lanes(i, s)]
                    at = OUT + 2 * (i - OUT) + half_of
                    z_copies[i, j].append(copy(src, dst, z_send.at[at, j - 1], z_recv.at[at, j - 1], z_at(j)))
            for one in z_copies[i, j]:
                one.start()

    part = rows // 2
    toks = {}

    def tok_place(side, h, from_tp):
        return tok_all.at[side, pl.ds(h * part, part), aligned(from_tp, half)]

    def tok_z(h):
        toks[h] = copy(
            tok_ref.at[pl.ds(h * part, part), :], tok_place(b, h, t), tok_sem_s.at[h], tok_sem_r.at[h], z_peer
        )
        toks[h].start()

    to_partner = copy(tok_ref, tok_all.at[b, :, aligned(t, half)], tok_sem_s.at[4], tok_sem_r.at[4], partner)
    to_partner.start()
    spike_copy = copy(spike_ref, spikes.at[b], misc_s.at[0], misc_r.at[0], z_peer)
    spike_copy.start()
    for i in range(OUT - 1):
        z_send_piece(i)
    tok_z(0)
    z_send_piece(OUT - 1)
    tok_z(1)
    for i in range(OUT, OUT + splits):
        z_send_piece(i)

    def region(i, src, of_line, side=None):
        if i < OUT:
            begin = src * depth + of_line * piece
            if side is not None and piece % 32 == 0:
                count = piece // 2
                return w_all.at[i, pl.ds(pl.multiple_of(begin + side * count, count), count), :]
            lanes = slice(None) if side is None else pl.ds(side * (wide // 2), wide // 2)
            return w_all.at[i, pl.ds(pl.multiple_of(begin, piece), piece), lanes]
        which = slice(None) if side is None else pl.ds(side, 1)
        return wo_all.at[which, aligned(of_line, out_piece), out_lanes(i, src)]

    x_copies, y_copies, a_copies, b_copies = {}, {}, {}, {}

    def source(j):
        return lax.rem(s + ring - j, ring)

    def first_stage(i):
        for j in z_span:
            for one in z_copies[i, j]:
                one.wait_recv()
            block = region(i, source(j), line)
            for a in x_span:
                x_copies[i, j, a] = copy(block, block, x_send.at[i, j - 1, a - 1], x_recv.at[i, j - 1, a - 1], x_at(a))
                x_copies[i, j, a].start()
            for c in y_span:
                y_copies[i, j, c] = copy(block, block, y_send.at[i, j - 1, c - 1], y_recv.at[i, j - 1, c - 1], y_at(c))
                y_copies[i, j, c].start()

    def second_stage(i):
        for j in z_span:
            for a in x_span:
                x_copies[i, j, a].wait_recv()
                behind = g * across + lax.rem(f + across - a, across)
                block = region(i, source(j), behind, 0)
                for c in y_span:
                    one = copy(block, block, a_send.at[i, j - 1, a - 1, c - 1], a_recv.at[i, j - 1, a - 1, c - 1], y_at(c))
                    one.start()
                    a_copies[i, j, a, c] = one
            for c in y_span:
                y_copies[i, j, c].wait_recv()
                behind = lax.rem(g + down - c, down) * across + f
                block = region(i, source(j), behind, 1)
                for a in x_span:
                    one = copy(block, block, b_send.at[i, j - 1, a - 1, c - 1], b_recv.at[i, j - 1, a - 1, c - 1], x_at(a))
                    one.start()
                    b_copies[i, j, a, c] = one

    def drain(i):
        for j in z_span:
            for a in x_span:
                for c in y_span:
                    a_copies[i, j, a, c].wait_recv()
                    b_copies[i, j, a, c].wait_recv()
        if i < OUT:
            local[2 + i].wait()

    def rows_at(start, count):
        return pl.ds(pl.multiple_of(start, CHUNK), count)

    def normalise(side, begin, count):
        step = 32

        @pl.loop(0, count // step)
        def _(r):
            block = tok_all[side, pl.ds(pl.multiple_of(begin + r * step, step), step), :].astype(F32)
            scale = lax.rsqrt(jnp.mean(block * block, axis=-1, keepdims=True) + EPS)
            span = pl.ds(pl.multiple_of(side * rows + begin + r * step, step), step)
            normed[span, :] = (block * scale * gain_ref[...]).astype(BF16)

        span = rows_at(side * rows + begin, count)
        block = normed[span, :]
        for w, gate_ref in enumerate((decay_ref, write_ref)):
            small[w, :, span] = mm_nt(gate_ref[...], block).astype(BF16).astype(F32)

    def project(i, start, count):
        span = rows_at(start, count)
        raw[i, span, :] = mm(normed[span, :], w_all[i]).astype(BF16)

    row_id = lax.broadcasted_iota(jnp.int32, (CHUNK, CHUNK), 0)
    col_id = lax.broadcasted_iota(jnp.int32, (CHUNK, CHUNK), 1)
    lower = row_id >= col_id
    strict = row_id > col_id
    eye = jnp.where(row_id == col_id, 1.0, 0.0)

    rows_ref[...] = jnp.zeros_like(rows_ref)

    def decays(side, begin, count):
        span = rows_at(side * rows + begin, count)
        for h in range(heads):
            head = (2 * t + b) * heads + h
            rate = jnp.exp(jnp.full((1, count), rate_ref[head], F32))
            spike = row_of(spikes[side, :, begin : begin + count], b * heads + h)
            rows_ref[h : h + 1, span] = -rate * softplus(row_of(small[0, :, span], head)) + spike
            level = row_of(small[1, :, span], head) + bias_ref[head]
            rows_ref[heads + h : heads + h + 1, span] = jax.nn.sigmoid(level)
        upper = jnp.where(row_id <= col_id, 1.0, 0.0)
        decay_row = lax.broadcasted_iota(jnp.int32, (rows_ref.shape[0], CHUNK), 0) < heads
        for c in range(count // CHUNK):
            lanes = rows_at(side * rows + begin + c * CHUNK, CHUNK)
            block = rows_ref[:, lanes]
            block = jnp.where(decay_row, mm(block, upper, HIGH), block)
            rows_ref[:, lanes] = block
            cols_ref[lanes, :] = jnp.concatenate([block, jnp.zeros((HEAD - block.shape[0], CHUNK), F32)], axis=0).T

    def units_of(start, count):
        first = start // CHUNK
        return [(h, first + c) for c in range(count // CHUNK) for h in range(heads)]

    def unit_of(u):
        return u[0], aligned(u[1], CHUNK)

    def slot(u):
        return u[1] * heads + u[0]

    def lanes_of(h):
        return slice(h * HEAD, (h + 1) * HEAD)

    def cum_col(u):
        h, span = unit_of(u)
        return cols_ref[span, h : h + 1]

    def beta_col(u):
        h, span = unit_of(u)
        return cols_ref[span, heads + h : heads + h + 1]

    def inverses(start, count):
        units = units_of(start, count)
        a = []
        for u in units:
            h, span = unit_of(u)
            keys = unit(silu(raw[0, span, lanes_of(h)].astype(F32)))
            diff = cum_col(u) - rows_ref[h : h + 1, span]
            gamma = jnp.where(lower, jnp.exp(jnp.where(lower, diff, 0.0)), 0.0)
            k_all[slot(u)] = keys
            gamma_all[slot(u)] = gamma
            a.append(jnp.where(strict, mm3(keys * beta_col(u), keys, mm_nt) * gamma, 0.0))
        size = 1
        inv = None
        while size < CHUNK:
            pair = 2 * size
            off = (row_id // pair == col_id // pair) & (row_id % pair >= size) & (col_id % pair < size)
            cross = [jnp.where(off, x, 0.0) for x in a]
            if inv is None:
                inv = [eye - x for x in cross]
            else:
                mid = [mm3(x, y) for x, y in zip(cross, inv)]
                inv = [y - mm3(y, x) for x, y in zip(mid, inv)]
            size = pair
        for u, x in zip(units, inv):
            t_all[slot(u)] = x

    def blocks(start, count):
        for u in units_of(start, count):
            h, span = unit_of(u)
            keys = k_all[slot(u)]
            query = unit(silu(raw[1, span, lanes_of(h)].astype(F32))) * HEAD ** (-0.5)
            values = silu(raw[2, span, lanes_of(h)].astype(F32))
            cum = cum_col(u)
            beta = beta_col(u)
            grow = jnp.exp(cum)
            last = cum[CHUNK - 1 :, :]
            right = jnp.concatenate([values * beta, keys * beta * grow], axis=1)
            solved = mm3(t_all[slot(u)], right)
            q_k = mm1(query, keys, mm_nt) * gamma_all[slot(u)]
            inner = mm1(q_k, solved)
            p_all[slot(u)] = query * grow - inner[:, HEAD:]
            u_all[slot(u)] = inner[:, :HEAD]
            state = mm3(keys * jnp.exp(last - cum), solved, mm_tn)
            m_all[slot(u)] = eye * jnp.exp(last) - state[:, HEAD:]
            o_all[slot(u)] = state[:, :HEAD]

    def recurrence():
        for h in range(heads):
            p_out[h, :CHUNK, :] = p_all[h]
            u_out[h, :CHUNK, :] = u_all[h]
        x = [jnp.concatenate([o_all[h], m_all[h]], axis=1) for h in range(heads)]
        for c in range(1, chunks):
            span = slice(c * CHUNK, (c + 1) * CHUNK)
            for h in range(heads):
                u = c * heads + h
                out = mm1(p_all[u], x[h])
                u_out[h, span, :] = out[:, :HEAD] + u_all[u]
                p_out[h, span, :] = out[:, HEAD:]
                nxt = mm3(m_all[u], x[h])
                x[h] = jnp.concatenate([nxt[:, :HEAD] + o_all[u], nxt[:, HEAD:]], axis=1)
        for h in range(heads):
            x_end[h] = x[h]

    state_copy = copy(st_send, st_recv, misc_s.at[1], misc_r.at[1], ahead)

    def send_state():
        @pl.when(s + 2 < ring)
        def _():
            for h in range(heads):
                st_send[h] = (x_end[h, :, :HEAD] + mm3(x_end[h, :, HEAD:], st_first[h])).astype(BF16)
            state_copy.start()

    rim_copy = copy(tail, rim, misc_s.at[2], misc_r.at[2], ahead)

    def gated():
        @pl.loop(0, pos // CHUNK)
        def _(r):
            span = aligned(r, CHUNK)
            glu = raw[3, span, :].astype(F32) * jax.nn.sigmoid(raw[4, span, :].astype(F32))
            ext[pl.ds(pl.multiple_of(pad + r * CHUNK, pad), CHUNK), :] = glu.astype(BF16).astype(F32)

        @pl.when(s + 2 < ring)
        def _():
            tail[...] = ext[pos:, :].astype(BF16)
            rim_copy.start()

    my_chan = pl.ds(pl.multiple_of((2 * t + b) * wide, wide), wide)
    step = 64
    lane = lax.broadcasted_iota(jnp.int32, (step, HEAD), 1)

    def convolve(r):
        acc = jnp.zeros((step, wide), F32)
        window = ext[pl.ds(pl.multiple_of(r * step, step), step + pad), :]
        first = pad - tap_count + 1
        for phase in range(8):
            offsets = [o for o in range(first, first + tap_count) if o % 8 == phase]
            shifted = window[phase : offsets[-1] + step]
            for o in offsets:
                tap = taps_ref[o - first : o - first + 1, my_chan]
                acc = acc + tap * shifted[o - phase : o - phase + step]
        conv_ref[aligned(r, step), :] = acc
        total = jnp.sum(acc, axis=-1, keepdims=True)
        squares = jnp.sum(acc * acc, axis=-1, keepdims=True)
        stat_ref[aligned(r, step), :] = jnp.where(lane == 0, total, jnp.where(lane == 1, squares, 0.0))

    mine = b * rows
    peers = (1 - b) * rows
    peers_late = peers + part
    forwards = []

    def forward_tok(h):
        toks[h].wait_recv()
        block = tok_place(1 - b, h, t)
        one = copy(block, block, tok_sem_s.at[2 + h], tok_sem_r.at[2 + h], partner)
        one.start()
        forwards.append(one)

    local[0].wait()
    local[1].wait()
    to_partner.wait_recv()
    normalise(b, 0, rows)
    decays(b, 0, rows)
    first_stage(0)
    first_stage(1)
    second_stage(0)
    first_stage(2)
    second_stage(1)
    first_stage(3)
    drain(0)
    project(0, mine, rows)
    inverses(mine, rows)
    second_stage(2)
    forward_tok(0)
    drain(1)
    project(1, mine, rows)
    spike_copy.wait_recv()
    forwards[0].wait_recv()
    normalise(1 - b, 0, part)
    decays(1 - b, 0, part)
    first_stage(4)
    second_stage(3)
    drain(2)
    project(2, mine, rows)
    blocks(mine, rows)
    for i in range(3):
        project(i, peers, part)
    inverses(peers, part)
    forward_tok(1)
    second_stage(4)
    blocks(peers, part)
    forwards[1].wait_recv()
    normalise(1 - b, part, part)
    decays(1 - b, part, part)
    for i in range(3):
        project(i, peers_late, part)
    first_stage(OUT)
    inverses(peers_late, part)
    drain(3)
    project(3, mine, rows)
    project(3, peers, rows)
    drain(4)
    project(4, mine, rows)
    project(4, peers, rows)
    gated()
    for i in range(OUT + 1, OUT + splits):
        first_stage(i)
    blocks(peers_late, part)
    recurrence()

    @pl.when(s < 2)
    def _():
        for h in range(heads):
            st_first[h] = state_ref[b * heads + h]
        send_state()

    @pl.loop(1, pos // step)
    def _(r):
        convolve(r)

    second_stage(OUT)

    @pl.when(s < 2)
    def _():
        ext[:pad, :] = jnp.zeros((pad, wide), F32)

    @pl.when(s >= 2)
    def _():
        rim_copy.wait_recv()
        ext[:pad, :] = rim[...].astype(F32)

    convolve(0)
    sums[0] = stat_ref[...].T[: sums.shape[1]]
    sum_copies = [
        copy(sums.at[0], sums.at[1 + d], sum_s.at[d], sum_r.at[d], peer)
        for d, peer in enumerate((partner, z_peer, far))
    ]
    for one in sum_copies:
        one.start()

    @pl.when(s >= 2)
    def _():
        state_copy.wait_recv()
        for h in range(heads):
            st_first[h] = st_recv[h].astype(F32)
        send_state()

    for h in range(heads):
        attn = mm1(p_out[h], st_first[h]) + u_out[h]
        attn = attn * lax.rsqrt(jnp.mean(attn * attn, axis=-1, keepdims=True) + EPS) * head_gain_ref[...]
        mix[:, lanes_of(h)] = attn.astype(BF16)

    for one in sum_copies:
        one.wait_recv()
    total = sums[0] + sums[1] + sums[2] + sums[3]
    mean = total[0:1] / channels
    scale = lax.rsqrt(total[1:2] / channels - mean * mean + EPS)
    stats = jnp.concatenate([mean, scale, jnp.zeros((HEAD - 2, pos), F32)], axis=0)
    stat_ref[...] = stats.T

    @pl.loop(0, pos // step)
    def _(r):
        span = aligned(r, step)
        stat = stat_ref[span, :]
        value = (conv_ref[span, :] - stat[:, 0:1]) * stat[:, 1:2] * chan_gain_ref[:, my_chan]
        mix[span, wide:] = silu(value).astype(BF16)

    for i in range(OUT + 1, OUT + splits):
        second_stage(i)
    for one in local[2 + OUT :]:
        one.wait()

    def product(side, at, of_tp):
        block = mix[aligned(side, rows), :]
        lanes = pl.ds(pl.multiple_of(of_tp * half + at * width, width), width)
        return mm(block[:, :wide], wo_all[0, :, lanes]) + mm(block[:, wide:], wo_all[1, :, lanes])

    order = [(k, p, m) for k in range(splits) for p in range(2) for m in range(turns)]
    pairs, z_outs = {}, {}

    def give(k, p, m):
        if p == 0 and m == 0:
            drain(OUT + k)
        at = m * splits + k
        to_pair[p, at] = product(1 - b if p == 0 else b, at, 1 - t).astype(BF16)
        pairs[p, at] = copy(to_pair.at[p, at], from_pair.at[p, at], pair_s.at[p, at], pair_r.at[p, at], partner)
        pairs[p, at].start()

    def finish(at):
        z_outs[at].wait_recv()
        out_ref[:, at * width : (at + 1) * width] = (own_sum[at] + from_z[at].astype(F32)).astype(BF16)

    give(*order[0])
    for n, (k, p, m) in enumerate(order):
        if n + 1 < len(order):
            give(*order[n + 1])
        at = m * splits + k
        value = product(1 - b if p == 0 else b, at, t)
        pairs[p, at].wait_recv()
        value = value + from_pair[p, at].astype(F32)
        if p == 0:
            to_z[at] = value.astype(BF16)
            z_outs[at] = copy(to_z.at[at], from_z.at[at], zo_s.at[at], zo_r.at[at], z_peer)
            z_outs[at].start()
        else:
            own_sum[at] = value
    for k in range(splits):
        for m in range(turns):
            finish(m * splits + k)

    for ones in z_copies.values():
        for one in ones:
            one.wait_send()
    for group_of in (x_copies, y_copies, a_copies, b_copies, toks, pairs, z_outs):
        for one in group_of.values():
            one.wait_send()
    for one in [to_partner, spike_copy] + forwards + sum_copies:
        one.wait_send()

    @pl.when(s + 2 < ring)
    def _():
        state_copy.wait_send()
        rim_copy.wait_send()


def layer(sizes, tokens, weights, outs, spikes, states, decay_gates, write_gates, gain, rate, bias, head_gain, taps, chan_gain):
    across, ring, down = sizes
    rows, half = tokens.shape
    depth, wide_tp = weights[0].shape
    wide = wide_tp // 2
    heads = wide // HEAD
    pos = 2 * rows
    chunks = pos // CHUNK
    units = chunks * heads
    total = 2 * half
    pad = -(-(taps.shape[0] - 1) // 32) * 32
    width = min(256, outs[0].shape[1])
    parts = half // width
    dma = pltpu.SemaphoreType.DMA
    vmem = pl.BlockSpec(memory_space=pltpu.VMEM)
    smem = pl.BlockSpec(memory_space=pltpu.SMEM)
    anywhere = pl.BlockSpec(memory_space=pl.ANY)
    scratch = pltpu.VMEM
    square = (units, CHUNK, HEAD)
    splits = outs[0].shape[1] // width
    pieces, spread = 5 + 2 * splits, 5 + splits
    hops, x_hops, y_hops = (max(size - 1, 1) for size in (ring, across, down))
    return pl.pallas_call(
        functools.partial(layer_kernel, sizes),
        out_shape=jax.ShapeDtypeStruct((rows, half), BF16),
        in_specs=[anywhere] * 8 + [vmem] * 5 + [smem] * 2 + [vmem] * 3,
        out_specs=vmem,
        scratch_shapes=[
            scratch((2, rows, total), BF16),
            scratch((pos, total), BF16),
            scratch((5, depth * ring, wide), BF16),
            scratch((2, wide, total), BF16),
            scratch((5, pos, wide), BF16),
            scratch((2,) + spikes.shape, F32),
            scratch((2, decay_gates.shape[0], pos), F32),
            scratch((8, pos), F32),
            scratch((pos, HEAD), F32),
            scratch((units, CHUNK, CHUNK), F32),
            scratch(square, F32),
            scratch((units, CHUNK, CHUNK), F32),
            scratch(square, F32),
            scratch(square, F32),
            scratch((units, HEAD, HEAD), F32),
            scratch((units, HEAD, HEAD), F32),
            scratch((heads, pos, HEAD), F32),
            scratch((heads, pos, HEAD), F32),
            scratch((heads, HEAD, 2 * HEAD), F32),
            scratch((heads, HEAD, HEAD), F32),
            scratch((heads, HEAD, HEAD), BF16),
            scratch((heads, HEAD, HEAD), BF16),
            scratch((pad + pos, wide), F32),
            scratch((pad, wide), BF16),
            scratch((pad, wide), BF16),
            scratch((pos, wide), F32),
            scratch((pos, HEAD), F32),
            scratch((4, 8, pos), F32),
            scratch((pos, 2 * wide), BF16),
            scratch((2, parts, rows, width), BF16),
            scratch((2, parts, rows, width), BF16),
            scratch((parts, rows, width), BF16),
            scratch((parts, rows, width), BF16),
            scratch((parts, rows, width), F32),
            dma((pieces, hops)), dma((pieces, hops)),
            dma((spread, hops, x_hops)), dma((spread, hops, x_hops)),
            dma((spread, hops, y_hops)), dma((spread, hops, y_hops)),
            dma((spread, hops, x_hops, y_hops)), dma((spread, hops, x_hops, y_hops)),
            dma((spread, hops, x_hops, y_hops)), dma((spread, hops, x_hops, y_hops)),
            dma((5,)), dma((5,)), dma((3,)), dma((3,)), dma((3,)), dma((3,)),
            dma((2, parts)), dma((2, parts)), dma((parts,)), dma((parts,)),
            dma((9,)),
        ],
        compiler_params=pltpu.CompilerParams(
            collective_id=1, has_side_effects=True, vmem_limit_bytes=56 * 1024 * 1024
        ),
        name="layer",
    )(tokens, *weights, *outs, spikes, states, decay_gates, write_gates, gain, rate, bias, head_gain, taps, chan_gain)


def on_device(
    tokens,
    input_norm_gain,
    query_weight,
    key_weight,
    value_weight,
    decay_gate_weight,
    write_strength_weight,
    up_weight,
    gate_half_weight,
    log_decay_rate,
    write_strength_bias,
    decay_spike_added,
    starting_state,
    head_norm_gain,
    convolution_kernel,
    channel_norm_gain,
    delta_output_rows,
    convolution_output_rows,
):
    sizes = (lax.axis_size("fs"), lax.axis_size("sp"), lax.axis_size("grp"))
    return layer(
        sizes,
        tokens[0],
        (query_weight, key_weight, value_weight, up_weight, gate_half_weight),
        (delta_output_rows, convolution_output_rows),
        decay_spike_added[0].T,
        starting_state[0],
        decay_gate_weight.T,
        write_strength_weight.T,
        input_norm_gain[None],
        log_decay_rate,
        write_strength_bias,
        head_norm_gain[None],
        convolution_kernel,
        channel_norm_gain[None],
    )[None]


def solution(mesh):
    return jax.shard_map(
        on_device,
        mesh=mesh,
        in_specs=(
            P(("grp", "fs"), "sp", "tp"),
            P(),
            P("sp", "tp"),
            P("sp", "tp"),
            P("sp", "tp"),
            P(),
            P(),
            P("sp", "tp"),
            P("sp", "tp"),
            P(),
            P(),
            P(("grp", "fs"), "sp", "tp"),
            P(("grp", "fs"), "tp", None, None),
            P(),
            P(),
            P(),
            P("tp", "sp"),
            P("tp", "sp"),
        ),
        out_specs=P(("grp", "fs"), "sp", "tp"),
        check_vma=False,
    )
```
